128 devices in a mesh: sp: 32 (over z, y, core), tp: 4 (over x).
Axes of the slice: x: 4, y: 4, z: 4, core: 2. Of those that a mesh axis runs over, the one named last changes fastest.
Arguments:
- conv_input: bfloat16 [16384, 1024], P('sp', 'tp'), may hold values from -6 to 6
- gate_inner: bfloat16 [16384, 1024], P('sp', 'tp'), may hold values from -6 to 6
- gate_outer: bfloat16 [16384, 1024], P('sp', 'tp'), may hold values from -6 to 6
- conv_taps: bfloat16 [3, 1024], P(None, 'tp'), may hold values from -3.5 to 3.5
- doc_ids: int32 [16384], P('sp'), may hold values from 0 to 15, never falling along the last dimension, each value on 1 to 2048 neighbouring positions
- residual_in: bfloat16 [16384, 2048], P(('sp', 'tp')), may hold values from -6 to 6
- out_proj: bfloat16 [1024, 2048], replicated, may hold values from -0.1875 to 0.1875
- norm_gain: float32 [2048], replicated, may hold values from 0.1 to 1.9
- expert_ids: int32 [16384, 2], P(('sp', 'tp')), may hold values from 0 to 127, all different within a row; in each aligned block of 128 rows (0 to 127, 128 to 255, ...) at most 4 rows name the same one
- expert_weights: float32 [16384, 2], P(('sp', 'tp')), may hold values from 0.2 to 1
- gate_proj: bfloat16 [128, 2048, 1024], P(('sp', 'tp')), may hold values from -0.125 to 0.125
- up_proj: bfloat16 [128, 2048, 1024], P(('sp', 'tp')), may hold values from -0.125 to 0.125
- down_proj: bfloat16 [128, 1024, 2048], P(('sp', 'tp')), may hold values from -0.1875 to 0.1875
Outputs:
- layer_out: bfloat16 [16384, 2048], P(('sp', 'tp'))
The draws below stay inside these ranges and needn't reach their ends.
Inputs may be any that keep to these rules, and one draw needn't show every extreme that they name: `doc_ids`: never falls along positions; each document has at most 2048 positions. `expert_ids`: each row names 2 different experts; within the rows of one device, aligned blocks of 128 rows, no expert is named more than 4 times, a bound that some block reaches.
All inputs are finite; a program needn't handle non-finite values.
Results may differ from the reference program's by a relative error of at most 0.009.
Values may be sent and summed in bfloat16 or wider, within the bound.
A program may use at most 64 MiB of HBM per device.

```python
import math
import jax
import jax.numpy as jnp
import numpy as np
from jax import lax

D = 2048
CONV = 1024
FF = 1024
KTAPS = 3
TOPK = 2
TOKENS = 16384
ROWS = 128
EXPERTS = 128
CAP = 4
NDOCS = 16
DOC_MOST = 2048


def steps_of(key, shape, cuts, low, top_value):
    level = 1.0
    for axis_at, shards_of in cuts:
        heights = jax.random.uniform(jax.random.fold_in(jax.random.fold_in(key, 6), axis_at), (shards_of,), jnp.float32, low / len(cuts), top_value / len(cuts))
        level = level * jnp.repeat(jnp.exp(heights), shape[axis_at] // shards_of).reshape((-1,) + (1,) * (len(shape) - 1 - axis_at))
    return level


def length_profile(amount, total, most, skew):
    loads = [(1 << 20) // math.isqrt(standing ** skew) + 1 for standing in range(2, amount + 1)]
    surplus, given = total - most - (amount - 1), [1] * (amount - 1)
    while surplus > 0:
        free = [i for i in range(amount - 1) if given[i] < most]
        pool, left = sum([loads[i] for i in free]), surplus
        for i in free:
            more = min(most - given[i], max(1, left * loads[i] // pool), surplus)
            given[i] = given[i] + more
            surplus = surplus - more
    return np.array([most] + given)


def uneven(stream_key, number_of, total, most, slope):
    if number_of == 2:
        one = jax.random.randint(stream_key, (), max(1, total - most), min(most, total - 1) + 1)
        return jnp.stack([one, total - one])
    lengths = jnp.asarray(length_profile(number_of, total, most, slope), jnp.int32)
    twos = (number_of - 1) // 2
    giver, taker = lengths[1:1 + 2 * twos:2], lengths[2:2 + 2 * twos:2]
    slack = jnp.minimum(giver - 1, most - taker)
    shifted = jax.random.randint(jax.random.fold_in(stream_key, 1), (twos,), 0, 1 << 20) % (slack + 1)
    lengths = lengths.at[1:1 + 2 * twos:2].set(giver - shifted).at[2:2 + 2 * twos:2].set(taker + shifted)
    return lengths[jax.random.permutation(jax.random.fold_in(stream_key, 2), number_of)]


def routed_block(rng, own, number, rows, number_of, top, reach, slope):
    ranking = jax.random.permutation(rng, number_of)
    heavy_load, common = portions_of(number_of, rows * top, reach, slope, True), portions_of(number_of, rows * top, reach, slope, False)
    places = jnp.arange(number_of)

    def named(lengths, offset_by):
        used = int((lengths > 0).sum())
        fixed = max(1, used // 4)
        shifted = fixed + (places - fixed + offset_by * (used - fixed)) % max(1, number_of - fixed)
        return jnp.zeros((number_of,), jnp.int32).at[ranking[jnp.where(places < fixed, places, shifted)]].set(jnp.asarray(lengths, jnp.int32))

    lengths = jnp.where(number % 4 == 0, named(heavy_load, number // 4), named(common, number - number // 4 - 1))
    mixed = jax.random.permutation(jax.random.fold_in(own, 3), number_of)
    source_of, taker = mixed[0:number_of // 2 * 2:2], mixed[1:number_of // 2 * 2:2]
    slack = jnp.minimum(lengths[source_of] - 1, reach - lengths[taker]) // 2
    slack = jnp.where((source_of == ranking[0]) | (taker == ranking[0]) | (lengths[taker] == 0), 0, jnp.maximum(slack, 0))
    shifted = jax.random.randint(jax.random.fold_in(own, 4), (number_of // 2,), 0, 1 << 20) % (slack + 1)
    lengths = lengths.at[source_of].add(-shifted).at[taker].add(shifted)
    members = jnp.searchsorted(jnp.cumsum(lengths), jnp.arange(rows * top), side="right").astype(jnp.int32)
    table = members.reshape(top, rows).T
    table = table[jax.random.permutation(jax.random.fold_in(own, 1), rows)]
    offset_by = jax.random.randint(jax.random.fold_in(own, 2), (rows, 1), 0, top)
    return jnp.take_along_axis(table, (jnp.arange(top)[None, :] + offset_by) % top, axis=1)


def portions_of(amount, total, limit, skew, full):
    portions = [(1 << 20) // math.isqrt(rank ** skew) + 1 for rank in range(1, amount + 1)]
    largest = limit if full else min(limit, max(-(-total // amount), total * portions[0] // sum(portions)))
    least = 1 if total - largest >= amount - 1 else 0
    counts, rest = [largest] + [least] * (amount - 1), total - largest - least * (amount - 1)
    while rest > 0:
        free = [i for i in range(1, amount) if counts[i] < largest] or [i for i in range(1, amount) if counts[i] < limit]
        whole, budget = sum([portions[i] for i in free]), rest
        for i in free:
            extra = min(limit - counts[i], max(1, budget * portions[i] // whole), rest)
            counts[i] = counts[i] + extra
            rest = rest - extra
    return np.array(counts)


def gaussian(rng, dims, scale, reach, pieces=(), kind=jnp.bfloat16):
    result = jax.random.normal(rng, dims, jnp.float32) * scale
    if len(pieces) > 0:
        result = steps_of(rng, dims, pieces, -0.22, 0.18) * result
    return jnp.clip(result, min=-reach, max=reach).astype(kind)


def setup_inputs(seed: int = 0) -> dict:
    splits = jax.random.split(jax.random.key(seed), 14)
    conv_input = gaussian(splits[0], (TOKENS, CONV), 1.0, 6.0, ((0, 32), (1, 4)))
    gate_inner = gaussian(splits[1], (TOKENS, CONV), 1.0, 6.0, ((0, 32), (1, 4)))
    gate_outer = gaussian(splits[2], (TOKENS, CONV), 1.0, 6.0, ((0, 32), (1, 4)))
    conv_taps = gaussian(splits[3], (KTAPS, CONV), KTAPS ** -0.5, 3.5, ((1, 4),))
    doc_ids = jnp.searchsorted(jnp.cumsum(uneven(splits[4], NDOCS, TOKENS, DOC_MOST, 0)), jnp.arange(TOKENS), side="right").astype(jnp.int32)
    residual_in = gaussian(splits[5], (TOKENS, D), 1.0, 6.0, ((0, 128),))
    out_proj = gaussian(splits[6], (CONV, D), CONV ** -0.5, 0.1875)
    norm_gain = jnp.clip(1.0 + 0.18 * jax.random.normal(splits[7], (D,), jnp.float32), 0.1, 1.9)
    expert_ids_keys = jax.random.split(jax.random.fold_in(splits[8], 1), TOKENS // ROWS)
    expert_ids_turns = jax.random.permutation(jax.random.fold_in(splits[8], 3), TOKENS // ROWS)
    expert_ids = jax.vmap(lambda own, number: routed_block(jax.random.fold_in(splits[8], 2), own, number, ROWS, EXPERTS, TOPK, CAP, 1))(expert_ids_keys, expert_ids_turns).reshape((TOKENS, TOPK))
    expert_weights = jnp.clip(0.2 + 0.8 * jax.random.uniform(splits[9], (TOKENS, TOPK), jnp.float32) ** steps_of(splits[9], (TOKENS, TOPK), ((0, 128),), -0.2, 0.2), 0.2, 1.0)
    gate_proj = gaussian(splits[10], (EXPERTS, D, FF), D ** -0.5, 0.125, ((0, 128),))
    up_proj = gaussian(splits[11], (EXPERTS, D, FF), D ** -0.5, 0.125, ((0, 128),))
    down_proj = gaussian(splits[12], (EXPERTS, FF, D), FF ** -0.5, 0.1875, ((0, 128),))
    return {"conv_input": conv_input, "gate_inner": gate_inner, "gate_outer": gate_outer, "conv_taps": conv_taps, "doc_ids": doc_ids, "residual_in": residual_in, "out_proj": out_proj, "norm_gain": norm_gain, "expert_ids": expert_ids, "expert_weights": expert_weights, "gate_proj": gate_proj, "up_proj": up_proj, "down_proj": down_proj}


def expert_rows(arrived, gate_weight, up_weight, down_weight):
    gate_value = jnp.dot(arrived, gate_weight, preferred_element_type=jnp.float32)
    up_value = jnp.dot(arrived, up_weight, preferred_element_type=jnp.float32)
    hidden = (jax.nn.silu(gate_value) * up_value).astype(jnp.bfloat16)
    return jnp.dot(hidden, down_weight, preferred_element_type=jnp.float32).astype(jnp.bfloat16)

def reference(conv_input, gate_inner, gate_outer, conv_taps, doc_ids, residual_in, out_proj, norm_gain, expert_ids, expert_weights, gate_proj, up_proj, down_proj):
    inner_prod = conv_input.astype(jnp.float32) * gate_inner.astype(jnp.float32)
    tap_values = conv_taps.astype(jnp.float32)
    channels = inner_prod.shape[1]
    one_rows = jnp.concatenate([jnp.zeros((1, channels), jnp.float32), inner_prod[:-1]], axis=0)
    two_rows = jnp.concatenate([jnp.zeros((2, channels), jnp.float32), inner_prod[:-2]], axis=0)
    one_docs = jnp.concatenate([jnp.full((1,), -1, jnp.int32), doc_ids[:-1]], axis=0)
    two_docs = jnp.concatenate([jnp.full((2,), -1, jnp.int32), doc_ids[:-2]], axis=0)
    one_back = jnp.where((one_docs == doc_ids)[:, None], one_rows, 0.0)
    two_back = jnp.where((two_docs == doc_ids)[:, None], two_rows, 0.0)
    mixed_rows = tap_values[2] * inner_prod + tap_values[1] * one_back + tap_values[0] * two_back
    conv_out = (gate_outer.astype(jnp.float32) * mixed_rows).astype(jnp.bfloat16)
    mix = jnp.dot(conv_out, out_proj, preferred_element_type=jnp.float32).astype(jnp.bfloat16)
    carried = residual_in.astype(jnp.float32) + mix.astype(jnp.float32)
    normed = (carried * lax.rsqrt(lax.optimization_barrier(jnp.mean(carried * carried, axis=1, keepdims=True)) + 1e-06) * norm_gain).astype(jnp.bfloat16)
    choose = expert_ids.shape[1]
    blocks = TOKENS // ROWS
    block_ids = expert_ids.reshape(blocks, ROWS * choose)
    onehot = (block_ids[:, :, None] == jnp.arange(EXPERTS, dtype=jnp.int32)[None, None, :]).astype(jnp.int32)
    slot_rank = lax.optimization_barrier(jnp.sum((jnp.cumsum(onehot, axis=1) - 1) * onehot, axis=2))
    block_index = jnp.arange(blocks, dtype=jnp.int32)[:, None]
    target = (block_ids * (blocks * CAP) + block_index * CAP + slot_rank).reshape(-1).astype(jnp.int32)
    sources = jnp.repeat(normed, choose, axis=0)
    buffer = jnp.zeros((EXPERTS * blocks * CAP, D), jnp.bfloat16).at[target].set(sources)
    buffer = buffer.reshape(EXPERTS, blocks * CAP, D)

    def serve(operands):
        return expert_rows(operands[0], operands[1], operands[2], operands[3])
    results = lax.map(serve, (buffer, gate_proj, up_proj, down_proj))
    picked = results.reshape(-1, D)[target].reshape(TOKENS, choose, D).astype(jnp.float32)
    combined = carried + lax.optimization_barrier(jnp.sum(expert_weights[:, :, None] * picked, axis=1))
    return combined.astype(jnp.bfloat16)
```

```python
import jax
import jax.numpy as jnp
from jax import lax
from jax.experimental import pallas as pl
from jax.experimental.pallas import tpu as pltpu
from jax.sharding import PartitionSpec as P

MESH = pl.DeviceIdType.MESH
BF = jnp.bfloat16
F32 = jnp.float32
NCH = 16
W = 128
HALF = (2,) * 5 + (8, W)
CUBE = (2,) * 6 + (8, W)


def gray_bits(v):
    return [(v // 2 + v % 2) % 2, v // 2]


def gray_flip(v, bit):
    return v + 1 - 2 * (v % 2) if bit == 0 else 3 - v


def layer_kernel(
    ci_h, gi_h, go_h, taps, docs, res_h, op_h, gain, ids, wts, wg_h, wu_h, wd_h,
    out,
    ci, gi, go, res, opv, wg, wu, wd,
    inner, halo, dhalo, docs8, conv_send, conv_all,
    carried, meta_send, meta, tok, pack, a_buf, land, gsum, usum, hid, y_buf, land2, comb,
    part_send, part_recv,
    load_sem, misc_send, misc_recv, tp_send, tp_recv, tok_send, tok_recv,
    d_send, d_recv, c_send, c_recv, p_send, p_recv,
):
    sp = lax.axis_index("sp")
    x = lax.axis_index("tp")
    c = sp % 2
    y = (sp // 2) % 4
    z = sp // 8
    mine = gray_bits(x) + gray_bits(y) + gray_bits(z)

    def neighbour(d):
        xx, yy, zz = x, y, z
        if d < 2:
            xx = gray_flip(x, d)
        elif d < 4:
            yy = gray_flip(y, d - 2)
        else:
            zz = gray_flip(z, d - 4)
        return ((zz * 4 + yy) * 2 + c, xx)

    nbr = [neighbour(d) for d in range(6)]
    twin = (sp + 1 - 2 * c, x)
    after = ((sp + 1) % 32, x)
    before = ((sp + 31) % 32, x)
    tp_far = [(sp, (x + j) % 4) for j in range(4)]

    def load(src, dst, i):
        return pltpu.make_async_copy(src, dst, load_sem.at[i])

    loads = [load(ci_h, ci, 0), load(gi_h, gi, 1), load(go_h, go, 2), load(res_h, res, 3),
             load(op_h, opv, 4), load(wg_h.at[0], wg, 5), load(wu_h.at[0], wu, 6), load(wd_h.at[0], wd, 7)]
    for i in range(3):
        loads[i].start()

    bar = pltpu.get_barrier_semaphore()
    for dev in nbr + [twin, tp_far[2], after, before]:
        pl.semaphore_signal(bar, inc=1, device_id=dev, device_id_type=MESH)

    meta_send[0:2, :] = ids[...].astype(F32)
    meta_send[2:4, :] = wts[...]
    docs8[1:5, :] = docs[...]

    for i in range(2):
        loads[i].wait()
    inner[8:520, :] = ci[...].astype(F32) * gi[...].astype(F32)
    loads[2].wait()
    for i in range(3, 8):
        loads[i].start()

    def remote(src, dst, ssem, rsem, dev):
        return pltpu.make_async_remote_copy(
            src_ref=src, dst_ref=dst, send_sem=ssem, recv_sem=rsem, device_id=dev, device_id_type=MESH
        )

    pl.semaphore_wait(bar, 10)
    halo_copy = remote(inner.at[pl.ds(512, 8)], halo, misc_send.at[0], misc_recv.at[0], after)
    doc_copy = remote(docs, dhalo, misc_send.at[1], misc_recv.at[1], after)
    meta_copy = remote(meta_send, meta, misc_send.at[2], misc_recv.at[2], twin)
    halo_copy.start()
    doc_copy.start()
    meta_copy.start()

    rows = lax.broadcasted_iota(jnp.int32, (128, 128), 0)
    lanes = lax.broadcasted_iota(jnp.int32, (128, 128), 1)
    eye = jnp.where(rows == lanes, 1.0, 0.0).astype(F32)

    def column(row):
        return jnp.sum(eye * row, axis=1, keepdims=True)

    t0 = taps[0:1, :].astype(F32)
    t1 = taps[1:2, :].astype(F32)
    t2 = taps[2:3, :].astype(F32)
    lane8 = lax.broadcasted_iota(jnp.int32, (8, 128), 1)

    def conv_block(b):
        cur = jnp.broadcast_to(docs8[b + 1 : b + 2, :], (8, 128))
        prev = jnp.broadcast_to(docs8[b : b + 1, :], (8, 128))
        one = jnp.where(lane8 < 1, pltpu.roll(prev, 1, 1), pltpu.roll(cur, 1, 1))
        two = jnp.where(lane8 < 2, pltpu.roll(prev, 2, 1), pltpu.roll(cur, 2, 1))
        m1 = column(jnp.where(one == cur, 1.0, 0.0).astype(F32)[0:1, :])
        m2 = column(jnp.where(two == cur, 1.0, 0.0).astype(F32)[0:1, :])
        base = 8 + 128 * b
        i0 = inner[base : base + 128, :]
        i1 = inner[base - 1 : base + 127, :]
        i2 = inner[base - 2 : base + 126, :]
        value = t2 * i0 + t1 * (m1 * i1) + t0 * (m2 * i2)
        gate = go[128 * b : 128 * b + 128, :].astype(F32)
        conv_send[b] = (gate * value).astype(BF)

    def tp_copy(b):
        slot = (b + 4 - x) % 4
        return remote(conv_send.at[b], conv_all.at[x], tp_send.at[slot], tp_recv.at[slot], (sp, b))

    for b in (1, 2, 3, 0):
        if b == 0:
            halo_copy.wait_recv()
            doc_copy.wait_recv()
            inner[0:8, :] = halo[...]
            docs8[0:1, :] = jnp.where(sp == 0, -1, dhalo[3:4, :])
        conv_block(b)

        @pl.when(x != b)
        def _():
            tp_copy(b).start()

        @pl.when(x == b)
        def _():
            conv_all[b] = conv_send[b]

    meta_copy.wait_recv()

    def routing(table):
        e = [table[a : a + 1, :] for a in range(2)]
        ec = [column(v) for v in e]
        out_rows = []
        for a in range(2):
            same = ((ec[0] == e[a]) | (ec[1] == e[a])) & (rows < lanes)
            rank = jnp.sum(jnp.where(same, 1.0, 0.0).astype(F32), axis=0, keepdims=True)
            ei = e[a].astype(jnp.int32)

            def gray(v):
                return v ^ (v >> 1)

            unit = gray(ei & 3) + 4 * gray((ei >> 3) & 3) + 16 * gray((ei >> 5) & 3)
            out_rows.append((unit * 8 + rank.astype(jnp.int32), (ei >> 2) & 1))
        return out_rows

    slot_rows = lax.broadcasted_iota(jnp.int32, (512, 128), 0)
    slot_lanes = lax.broadcasted_iota(jnp.int32, (128, 512), 1).astype(F32)
    for s, table in ((0, meta_send), (1, meta)):
        source_core = c if s == 0 else 1 - c
        targets = []
        for slot, parity in routing(table):
            targets.append(jnp.where(parity == c, slot + 4 * source_core, -1))
        hit = (slot_rows == targets[0]) | (slot_rows == targets[1])
        pack[:, 128 * s : 128 * s + 128] = jnp.where(hit, 1.0, 0.0).astype(F32).astype(BF)
        weight = jnp.zeros((128, 512), F32)
        for a in range(2):
            tc = column(targets[a].astype(F32))
            wc = column(table[2 + a : 3 + a, :])
            weight = weight + jnp.where(slot_lanes == tc, wc, 0.0)
        high = weight.astype(BF)
        comb[0, 128 * s : 128 * s + 128, :] = high
        comb[1, 128 * s : 128 * s + 128, :] = (weight - high.astype(F32)).astype(BF)

    loads[3].wait()
    loads[4].wait()
    for j in range(1, 4):
        pltpu.make_async_remote_copy(
            src_ref=conv_send.at[0], dst_ref=conv_all.at[(x + 4 - j) % 4], send_sem=tp_send.at[j],
            recv_sem=tp_recv.at[j], device_id=tp_far[j], device_id_type=MESH,
        ).wait_recv()
    total = jnp.zeros((128, 1), F32)
    for n in range(8):
        cols = slice(256 * n, 256 * n + 256)
        acc = jnp.zeros((128, 256), F32)
        for i in range(4):
            acc = acc + jnp.dot(conv_all[i], opv[256 * i : 256 * i + 256, cols], preferred_element_type=F32)
        value = res[:, cols].astype(F32) + acc.astype(BF).astype(F32)
        total = total + jnp.sum(value * value, axis=1, keepdims=True)
        carried[2 * n] = value[:, :128]
        carried[2 * n + 1] = value[:, 128:]
    scale = lax.rsqrt(total / 2048.0 + 1e-6)

    def tok_copy(j):
        ks = pl.ds(4 * j, 4)
        return remote(tok.at[ks, pl.ds(0, 128)], tok.at[ks, pl.ds(128, 128)], tok_send.at[j], tok_recv.at[j], twin)

    for k in range(NCH):
        tok[k, 0:128, :] = (carried[k] * scale * gain[:, W * k : W * k + W]).astype(BF)
        if k % 4 == 3:
            tok_copy(k // 4).start()

    def bit_view(buf, k, d, v):
        index = [slice(None)] * 6
        index[5 - d] = v
        return buf.at[(k, *index)]

    def swap(buf, landing, ss, rs, p, k):
        d = (k + p) % 6
        return remote(bit_view(buf, k, d, 1 - mine[d]), landing.at[d, k], ss.at[d, k], rs.at[d, k], nbr[d])

    def settle(buf, landing, ss, rs, p, k):
        d = (k + p) % 6
        copy = swap(buf, landing, ss, rs, p, k)
        copy.wait_recv()
        copy.wait_send()
        view = bit_view(buf, k, d, 1 - mine[d])
        view[...] = landing[d, k]

    def put(buf, k, value):
        buf[k] = value.reshape(CUBE).astype(BF)

    def pair(buf, k):
        both = [buf[k + i].astype(F32).reshape(512, W).astype(BF) for i in range(2)]
        return jnp.concatenate(both, axis=1)

    for k in range(0, NCH, 2):
        if k % 4 == 0:
            tok_copy(k // 4).wait_recv()
        source = jnp.concatenate([tok[k], tok[k + 1]], axis=1)
        packed = jnp.dot(pack[...], source, preferred_element_type=F32)
        for i in range(2):
            put(a_buf, k + i, packed[:, W * i : W * i + W])
            swap(a_buf, land, d_send, d_recv, 0, k + i).start()

    for p in range(1, 6):
        for k in range(NCH):
            settle(a_buf, land, d_send, d_recv, p - 1, k)
            swap(a_buf, land, d_send, d_recv, p, k).start()

    loads[5].wait()
    loads[6].wait()
    for k in range(0, NCH, 2):
        settle(a_buf, land, d_send, d_recv, 5, k)
        settle(a_buf, land, d_send, d_recv, 5, k + 1)
        source = pair(a_buf, k)
        rows_k = slice(W * k, W * k + 2 * W)
        for n in range(0, 1024, 512):
            g = jnp.dot(source, wg[rows_k, n : n + 512], preferred_element_type=F32)
            u = jnp.dot(source, wu[rows_k, n : n + 512], preferred_element_type=F32)
            if k == 0:
                gsum[:, n : n + 512] = g
                usum[:, n : n + 512] = u
            else:
                gsum[:, n : n + 512] += g
                usum[:, n : n + 512] += u

    @pl.loop(0, 16)
    def _(r):
        rs = pl.ds(pl.multiple_of(r * 32, 32), 32)
        g = gsum[rs, :]
        hid[rs, :] = (g / (1.0 + jnp.exp(-g)) * usum[rs, :]).astype(BF)

    loads[7].wait()
    for k in range(0, NCH, 2):
        result = jnp.dot(hid[...], wd[:, W * k : W * k + 2 * W], preferred_element_type=F32)
        for i in range(2):
            put(y_buf, k + i, result[:, W * i : W * i + W])
            swap(y_buf, land2, c_send, c_recv, 0, k + i).start()

    for p in range(1, 6):
        for k in range(NCH):
            settle(y_buf, land2, c_send, c_recv, p - 1, k)
            swap(y_buf, land2, c_send, c_recv, p, k).start()

    def part_copy(k):
        return remote(part_send.at[k], part_recv.at[k], p_send.at[k], p_recv.at[k], twin)

    for k in range(0, NCH, 2):
        settle(y_buf, land2, c_send, c_recv, 5, k)
        settle(y_buf, land2, c_send, c_recv, 5, k + 1)
        source = pair(y_buf, k)
        both = jnp.dot(comb[0], source, preferred_element_type=F32) + jnp.dot(
            comb[1], source, preferred_element_type=F32
        )
        for i in range(2):
            cols = slice(W * i, W * i + W)
            part_send[k + i] = both[128:, cols]
            part_copy(k + i).start()
            carried[k + i] += both[:128, cols]

    for k in range(NCH):
        part_copy(k).wait_recv()
        out[:, W * k : W * k + W] = (carried[k] + part_recv[k]).astype(BF)

    halo_copy.wait_send()
    doc_copy.wait_send()
    meta_copy.wait_send()
    for j in range(1, 4):
        pltpu.make_async_remote_copy(
            src_ref=conv_send.at[0], dst_ref=conv_all.at[0], send_sem=tp_send.at[j],
            recv_sem=tp_recv.at[j], device_id=tp_far[j], device_id_type=MESH,
        ).wait_send()
    for j in range(4):
        tok_copy(j).wait_send()
    for k in range(NCH):
        part_copy(k).wait_send()


def on_device(ci, gi, go, taps, docs, res, op, gain, ids, wts, wg, wu, wd):
    vmem = pl.BlockSpec(memory_space=pltpu.VMEM)
    hbm = pl.BlockSpec(memory_space=pl.ANY)
    dma = pltpu.SemaphoreType.DMA
    scratch = [
        pltpu.VMEM((512, 256), BF), pltpu.VMEM((512, 256), BF), pltpu.VMEM((512, 256), BF),
        pltpu.VMEM((128, 2048), BF), pltpu.VMEM((1024, 2048), BF),
        pltpu.VMEM((2048, 1024), BF), pltpu.VMEM((2048, 1024), BF), pltpu.VMEM((1024, 2048), BF),
        pltpu.VMEM((520, 256), F32), pltpu.VMEM((8, 256), F32), pltpu.VMEM((4, 128), jnp.int32),
        pltpu.VMEM((8, 128), jnp.int32), pltpu.VMEM((4, 128, 256), BF), pltpu.VMEM((4, 128, 256), BF),
        pltpu.VMEM((NCH, 128, W), F32), pltpu.VMEM((4, 128), F32), pltpu.VMEM((4, 128), F32),
        pltpu.VMEM((NCH, 256, W), BF), pltpu.VMEM((512, 256), BF),
        pltpu.VMEM((NCH, *CUBE), BF), pltpu.VMEM((6, NCH, *HALF), BF),
        pltpu.VMEM((512, 1024), F32), pltpu.VMEM((512, 1024), F32), pltpu.VMEM((512, 1024), BF),
        pltpu.VMEM((NCH, *CUBE), BF), pltpu.VMEM((6, NCH, *HALF), BF), pltpu.VMEM((2, 256, 512), BF),
        pltpu.VMEM((NCH, 128, W), F32), pltpu.VMEM((NCH, 128, W), F32),
        dma((8,)), dma((3,)), dma((3,)), dma((4,)), dma((4,)), dma((4,)), dma((4,)),
        dma((6, NCH)), dma((6, NCH)), dma((6, NCH)), dma((6, NCH)), dma((NCH,)), dma((NCH,)),
    ]
    return pl.pallas_call(
        layer_kernel,
        out_shape=jax.ShapeDtypeStruct((128, 2048), BF),
        in_specs=[hbm, hbm, hbm, vmem, vmem, hbm, hbm, vmem, vmem, vmem, hbm, hbm, hbm],
        out_specs=vmem,
        scratch_shapes=scratch,
        compiler_params=pltpu.CompilerParams(
            collective_id=0, has_side_effects=True, vmem_limit_bytes=64000000
        ),
    )(ci, gi, go, taps, docs.reshape(4, 128), res, op, gain.reshape(1, 2048), ids.T, wts.T, wg, wu, wd)


def solution(mesh):
    in_specs = (
        P("sp", "tp"),
        P("sp", "tp"),
        P("sp", "tp"),
        P(None, "tp"),
        P("sp"),
        P(("sp", "tp"), None),
        P(),
        P(),
        P(("sp", "tp"), None),
        P(("sp", "tp"), None),
        P(("sp", "tp"), None, None),
        P(("sp", "tp"), None, None),
        P(("sp", "tp"), None, None),
    )
    out_specs = P(("sp", "tp"), None)
    return jax.shard_map(
        on_device, mesh=mesh, in_specs=in_specs, out_specs=out_specs, check_vma=False
    )
```

```python
import jax
import jax.numpy as jnp
from jax import lax
from jax.experimental import pallas as pl
from jax.experimental.pallas import tpu as pltpu
from jax.sharding import PartitionSpec as P

MESH = pl.DeviceIdType.MESH
BF = jnp.bfloat16
F32 = jnp.float32
NCH = 8
W = 256
CUBE = (4, 4, 4, 8, W)
STEPS = (2, 1, 3)


def layer_kernel(
    ci_h, gi_h, go_h, taps, docs, res_h, op_h, gain, ids, wts, wg_h, wu_h, wd_h,
    out,
    ci, gi, go, res, opv, wg, wu, wd,
    inner, halo_send, halo_all, fix_send, fix_all, docs8, conv_send, conv_all,
    carried, meta_send, meta, tok, pack, there, gsum, usum, hid, back, comb,
    part_send, part_recv,
    load_sem, halo_s, halo_r, fix_s, fix_r, meta_s, meta_r, tp_send, tp_recv, tok_send, tok_recv,
    d_send, d_recv, c_send, c_recv, p_send, p_recv,
):
    sp = lax.axis_index("sp")
    x = lax.axis_index("tp")
    c = sp % 2
    y = (sp // 2) % 4
    z = sp // 8
    here = [z, y, x]

    def along(axis, step):
        at = [z, y, x]
        at[axis] = (at[axis] + step) % 4
        return ((at[0] * 4 + at[1]) * 2 + c, at[2])

    twin = (sp + 1 - 2 * c, x)
    after = ((sp + 1) % 32, 0)
    tp_far = [(sp, (x + j) % 4) for j in range(4)]

    def load(src, dst, i):
        return pltpu.make_async_copy(src, dst, load_sem.at[i])

    loads = [load(ci_h, ci, 0), load(gi_h, gi, 1), load(go_h, go, 2), load(res_h, res, 3),
             load(op_h, opv, 4), load(wg_h.at[0], wg, 5), load(wu_h.at[0], wu, 6), load(wd_h.at[0], wd, 7)]
    for i in range(3):
        loads[i].start()

    bar = pltpu.get_barrier_semaphore()
    for axis in range(3):
        for step in STEPS:
            pl.semaphore_signal(bar, inc=1, device_id=along(axis, step), device_id_type=MESH)
    pl.semaphore_signal(bar, inc=1, device_id=twin, device_id_type=MESH)

    @pl.when(x == 0)
    def _():
        for t in range(4):
            pl.semaphore_signal(bar, inc=1, device_id=((sp + 31) % 32, t), device_id_type=MESH)

    meta_send[0:2, :] = ids[...].astype(F32)
    meta_send[2:4, :] = wts[...]
    docs8[0:1, :] = jnp.full((1, 128), -1, jnp.int32)
    docs8[1:5, :] = docs[...]
    inner[0:8, :] = jnp.zeros((8, 256), F32)

    for i in range(2):
        loads[i].wait()
    inner[8:520, :] = ci[...].astype(F32) * gi[...].astype(F32)
    loads[2].wait()
    for i in range(3, 8):
        loads[i].start()

    def remote(src, dst, ssem, rsem, dev):
        return pltpu.make_async_remote_copy(
            src_ref=src, dst_ref=dst, send_sem=ssem, recv_sem=rsem, device_id=dev, device_id_type=MESH
        )

    t0 = taps[0:1, :].astype(F32)
    t1 = taps[1:2, :].astype(F32)
    t2 = taps[2:3, :].astype(F32)
    last = docs[3:4, :].astype(F32)
    halo_send[0:1, :] = t1 * inner[519:520, :]
    halo_send[1:2, :] = t0 * inner[518:519, :]
    halo_send[2:3, :] = t0 * inner[519:520, :]
    halo_send[3:4, :] = jnp.broadcast_to(last[:, 127:128], (1, 256))
    halo_send[4:5, :] = jnp.broadcast_to(last[:, 126:127], (1, 256))

    pl.semaphore_wait(bar, 11)
    halo_copy = remote(halo_send, halo_all.at[x], halo_s, halo_r.at[x], after)
    meta_copy = remote(meta_send, meta, meta_s, meta_r, twin)
    halo_copy.start()
    meta_copy.start()

    rows = lax.broadcasted_iota(jnp.int32, (128, 128), 0)
    lanes = lax.broadcasted_iota(jnp.int32, (128, 128), 1)
    eye = jnp.where(rows == lanes, 1.0, 0.0).astype(F32)

    def column(row):
        return jnp.sum(eye * row, axis=1, keepdims=True)

    lane8 = lax.broadcasted_iota(jnp.int32, (8, 128), 1)

    def conv_block(b):
        cur = jnp.broadcast_to(docs8[b + 1 : b + 2, :], (8, 128))
        prev = jnp.broadcast_to(docs8[b : b + 1, :], (8, 128))
        one = jnp.where(lane8 < 1, pltpu.roll(prev, 1, 1), pltpu.roll(cur, 1, 1))
        two = jnp.where(lane8 < 2, pltpu.roll(prev, 2, 1), pltpu.roll(cur, 2, 1))
        m1 = column(jnp.where(one == cur, 1.0, 0.0).astype(F32)[0:1, :])
        m2 = column(jnp.where(two == cur, 1.0, 0.0).astype(F32)[0:1, :])
        base = 8 + 128 * b
        i0 = inner[base : base + 128, :]
        i1 = inner[base - 1 : base + 127, :]
        i2 = inner[base - 2 : base + 126, :]
        value = t2 * i0 + t1 * (m1 * i1) + t0 * (m2 * i2)
        gate = go[128 * b : 128 * b + 128, :].astype(F32)
        conv_send[b] = (gate * value).astype(BF)
        if b == 0:
            fix_send[0:8, :] = value[0:8, :]
            fix_send[8:16, :] = gate[0:8, :]

    def tp_copy(b):
        slot = (b + 4 - x) % 4
        return remote(conv_send.at[b], conv_all.at[x], tp_send.at[slot], tp_recv.at[slot], (sp, b))

    def fix_copy(t):
        return remote(fix_send, fix_all.at[t], fix_s, fix_r.at[t], (sp, 0))

    for b in range(4):
        conv_block(b)

        @pl.when(x != b)
        def _():
            tp_copy(b).start()
            if b == 0:
                fix_copy(x).start()

        @pl.when(x == b)
        def _():
            conv_all[b] = conv_send[b]
            if b == 0:
                fix_all[0] = fix_send[...]

    meta_copy.wait_recv()

    def routing(table):
        e = [table[a : a + 1, :] for a in range(2)]
        ec = [column(v) for v in e]
        out_rows = []
        for a in range(2):
            same = ((ec[0] == e[a]) | (ec[1] == e[a])) & (rows < lanes)
            rank = jnp.sum(jnp.where(same, 1.0, 0.0).astype(F32), axis=0, keepdims=True)
            ei = e[a].astype(jnp.int32)

            unit = (ei & 3) + 4 * ((ei >> 3) & 3) + 16 * ((ei >> 5) & 3)
            out_rows.append((unit * 8 + rank.astype(jnp.int32), (ei >> 2) & 1))
        return out_rows

    slot_rows = lax.broadcasted_iota(jnp.int32, (512, 128), 0)
    slot_lanes = lax.broadcasted_iota(jnp.int32, (128, 512), 1).astype(F32)
    for s, table in ((0, meta_send), (1, meta)):
        source_core = c if s == 0 else 1 - c
        targets = []
        for slot, parity in routing(table):
            targets.append(jnp.where(parity == c, slot + 4 * source_core, -1))
        hit = (slot_rows == targets[0]) | (slot_rows == targets[1])
        pack[:, 128 * s : 128 * s + 128] = jnp.where(hit, 1.0, 0.0).astype(F32).astype(BF)
        weight = jnp.zeros((128, 512), F32)
        for a in range(2):
            tc = column(targets[a].astype(F32))
            wc = column(table[2 + a : 3 + a, :])
            weight = weight + jnp.where(slot_lanes == tc, wc, 0.0)
        high = weight.astype(BF)
        comb[0, 128 * s : 128 * s + 128, :] = high
        comb[1, 128 * s : 128 * s + 128, :] = (weight - high.astype(F32)).astype(BF)

    loads[3].wait()
    loads[4].wait()
    for j in range(1, 4):
        pltpu.make_async_remote_copy(
            src_ref=conv_send.at[0], dst_ref=conv_all.at[(x + 4 - j) % 4], send_sem=tp_send.at[j],
            recv_sem=tp_recv.at[j], device_id=tp_far[j], device_id_type=MESH,
        ).wait_recv()

    @pl.when(x == 0)
    def _():
        edge = lax.broadcasted_iota(jnp.int32, (8, 256), 0)
        first = docs[0:1, :].astype(F32)
        inside = jnp.where(sp == 0, 0.0, 1.0)
        for t in range(4):
            if t > 0:
                fix_copy(t).wait_recv()
            remote(halo_send, halo_all.at[t], halo_s, halo_r.at[t], after).wait_recv()
            from_behind = halo_all[t]
            m1 = jnp.where(from_behind[3:4] == first[:, 0:1], inside, 0.0)
            m2 = jnp.where(from_behind[4:5] == first[:, 0:1], inside, 0.0)
            m3 = jnp.where(from_behind[3:4] == first[:, 1:2], inside, 0.0)
            add0 = m1 * from_behind[0:1] + m2 * from_behind[1:2]
            add1 = m3 * from_behind[2:3]
            extra = jnp.where(edge == 0, add0, jnp.where(edge == 1, add1, 0.0))
            fixed = fix_all[t, 8:16, :] * (fix_all[t, 0:8, :] + extra)
            conv_all[t, 0:8, :] = fixed.astype(BF)

    total = jnp.zeros((128, 1), F32)
    for n in range(8):
        cols = slice(256 * n, 256 * n + 256)
        acc = jnp.zeros((128, 256), F32)
        for i in range(4):
            acc = acc + jnp.dot(conv_all[i], opv[256 * i : 256 * i + 256, cols], preferred_element_type=F32)
        value = res[:, cols].astype(F32) + acc.astype(BF).astype(F32)
        total = total + jnp.sum(value * value, axis=1, keepdims=True)
        carried[n] = value
    scale = lax.rsqrt(total / 2048.0 + 1e-6)

    def tok_copy(j):
        ks = pl.ds(2 * j, 2)
        return remote(tok.at[ks, pl.ds(0, 128)], tok.at[ks, pl.ds(128, 128)], tok_send.at[j], tok_recv.at[j], twin)

    for k in range(NCH):
        tok[k, 0:128, :] = (carried[k] * scale * gain[:, W * k : W * k + W]).astype(BF)
        if k % 2 == 1:
            tok_copy(k // 2).start()

    def plane(buf, p, k, axis, v):
        index = [slice(None)] * 3
        index[axis] = v
        return buf.at[(p, k, *index)]

    def move(buf, ss, rs, p, k, step):
        axis = (k + p) % 3
        return remote(
            plane(buf, p, k, axis, (here[axis] + step) % 4), plane(buf, p + 1, k, axis, here[axis]),
            ss.at[p, k, step - 1], rs.at[p, k, step - 1], along(axis, step),
        )

    def begin(buf, ss, rs, p, k):
        axis = (k + p) % 3
        for step in STEPS:
            move(buf, ss, rs, p, k, step).start()
        stay = plane(buf, p + 1, k, axis, here[axis])
        stay[...] = plane(buf, p, k, axis, here[axis])[...]

    def settle(buf, ss, rs, p, k):
        for step in STEPS:
            move(buf, ss, rs, p, k, step).wait_recv()

    def put(buf, k, value):
        buf[0, k] = value.reshape(CUBE).astype(BF)

    def rows_of(buf, k):
        return buf[3, k].astype(F32).reshape(512, W).astype(BF)

    for k in range(NCH):
        if k % 2 == 0:
            tok_copy(k // 2).wait_recv()
        put(there, k, jnp.dot(pack[...], tok[k], preferred_element_type=F32))
        begin(there, d_send, d_recv, 0, k)

    for p in range(1, 3):
        for k in range(NCH):
            settle(there, d_send, d_recv, p - 1, k)
            begin(there, d_send, d_recv, p, k)

    loads[5].wait()
    loads[6].wait()
    for k in range(NCH):
        settle(there, d_send, d_recv, 2, k)
        source = rows_of(there, k)
        rows_k = slice(W * k, W * k + W)
        for n in range(0, 1024, 512):
            g = jnp.dot(source, wg[rows_k, n : n + 512], preferred_element_type=F32)
            u = jnp.dot(source, wu[rows_k, n : n + 512], preferred_element_type=F32)
            if k == 0:
                gsum[:, n : n + 512] = g
                usum[:, n : n + 512] = u
            else:
                gsum[:, n : n + 512] += g
                usum[:, n : n + 512] += u

    @pl.loop(0, 16)
    def _(r):
        rs = pl.ds(pl.multiple_of(r * 32, 32), 32)
        g = gsum[rs, :]
        half = 0.5 * g
        hid[rs, :] = ((half + half * jnp.tanh(half)) * usum[rs, :]).astype(BF)

    loads[7].wait()
    for k in range(NCH):
        put(back, k, jnp.dot(hid[...], wd[:, W * k : W * k + W], preferred_element_type=F32))
        begin(back, c_send, c_recv, 0, k)

    for p in range(1, 3):
        for k in range(NCH):
            settle(back, c_send, c_recv, p - 1, k)
            begin(back, c_send, c_recv, p, k)

    def part_copy(k):
        return remote(part_send.at[k], part_recv.at[k], p_send.at[k], p_recv.at[k], twin)

    for k in range(NCH):
        settle(back, c_send, c_recv, 2, k)
        source = rows_of(back, k)
        both = jnp.dot(comb[0], source, preferred_element_type=F32) + jnp.dot(
            comb[1], source, preferred_element_type=F32
        )
        part_send[k] = both[128:]
        part_copy(k).start()
        carried[k] += both[:128]

    for k in range(NCH):
        part_copy(k).wait_recv()
        out[:, W * k : W * k + W] = (carried[k] + part_recv[k]).astype(BF)

    halo_copy.wait_send()
    meta_copy.wait_send()

    @pl.when(x != 0)
    def _():
        fix_copy(x).wait_send()

    for p in range(3):
        for k in range(NCH):
            for step in STEPS:
                move(there, d_send, d_recv, p, k, step).wait_send()
                move(back, c_send, c_recv, p, k, step).wait_send()
    for j in range(1, 4):
        pltpu.make_async_remote_copy(
            src_ref=conv_send.at[0], dst_ref=conv_all.at[0], send_sem=tp_send.at[j],
            recv_sem=tp_recv.at[j], device_id=tp_far[j], device_id_type=MESH,
        ).wait_send()
    for j in range(4):
        tok_copy(j).wait_send()
    for k in range(NCH):
        part_copy(k).wait_send()


def on_device(ci, gi, go, taps, docs, res, op, gain, ids, wts, wg, wu, wd):
    vmem = pl.BlockSpec(memory_space=pltpu.VMEM)
    hbm = pl.BlockSpec(memory_space=pl.ANY)
    dma = pltpu.SemaphoreType.DMA
    scratch = [
        pltpu.VMEM((512, 256), BF), pltpu.VMEM((512, 256), BF), pltpu.VMEM((512, 256), BF),
        pltpu.VMEM((128, 2048), BF), pltpu.VMEM((1024, 2048), BF),
        pltpu.VMEM((2048, 1024), BF), pltpu.VMEM((2048, 1024), BF), pltpu.VMEM((1024, 2048), BF),
        pltpu.VMEM((520, 256), F32), pltpu.VMEM((8, 256), F32), pltpu.VMEM((4, 8, 256), F32),
        pltpu.VMEM((16, 256), F32), pltpu.VMEM((4, 16, 256), F32),
        pltpu.VMEM((8, 128), jnp.int32), pltpu.VMEM((4, 128, 256), BF), pltpu.VMEM((4, 128, 256), BF),
        pltpu.VMEM((NCH, 128, W), F32), pltpu.VMEM((4, 128), F32), pltpu.VMEM((4, 128), F32),
        pltpu.VMEM((NCH, 256, W), BF), pltpu.VMEM((512, 256), BF), pltpu.VMEM((4, NCH, *CUBE), BF),
        pltpu.VMEM((512, 1024), F32), pltpu.VMEM((512, 1024), F32), pltpu.VMEM((512, 1024), BF),
        pltpu.VMEM((4, NCH, *CUBE), BF), pltpu.VMEM((2, 256, 512), BF),
        pltpu.VMEM((NCH, 128, W), F32), pltpu.VMEM((NCH, 128, W), F32),
        dma((8,)), dma, dma((4,)), dma, dma((4,)), dma, dma, dma((4,)), dma((4,)), dma((4,)), dma((4,)),
        dma((3, NCH, 3)), dma((3, NCH, 3)), dma((3, NCH, 3)), dma((3, NCH, 3)), dma((NCH,)), dma((NCH,)),
    ]
    return pl.pallas_call(
        layer_kernel,
        out_shape=jax.ShapeDtypeStruct((128, 2048), BF),
        in_specs=[hbm, hbm, hbm, vmem, vmem, hbm, hbm, vmem, vmem, vmem, hbm, hbm, hbm],
        out_specs=vmem,
        scratch_shapes=scratch,
        compiler_params=pltpu.CompilerParams(
            collective_id=0, has_side_effects=True, vmem_limit_bytes=64000000
        ),
    )(ci, gi, go, taps, docs.reshape(4, 128), res, op, gain.reshape(1, 2048), ids.T, wts.T, wg, wu, wd)


def solution(mesh):
    in_specs = (
        P("sp", "tp"),
        P("sp", "tp"),
        P("sp", "tp"),
        P(None, "tp"),
        P("sp"),
        P(("sp", "tp"), None),
        P(),
        P(),
        P(("sp", "tp"), None),
        P(("sp", "tp"), None),
        P(("sp", "tp"), None, None),
        P(("sp", "tp"), None, None),
        P(("sp", "tp"), None, None),
    )
    out_specs = P(("sp", "tp"), None)
    return jax.shard_map(
        on_device, mesh=mesh, in_specs=in_specs, out_specs=out_specs, check_vma=False
    )
```

```python
import jax
import jax.numpy as jnp
from jax import lax
from jax.experimental import pallas as pl
from jax.experimental.pallas import tpu as pltpu
from jax.sharding import PartitionSpec as P

MESH = pl.DeviceIdType.MESH
BF = jnp.bfloat16
F32 = jnp.float32
NCH = 4
W = 512
PARTS = 1
TOKS = 1
PIECES = NCH * PARTS
PW = W // PARTS
CUBE = (2, 4, 4, 8, PW)
HALF = 256
STEPS = (2, 1, 3)


def schedule():
    ks, ts = range(NCH), range(PIECES)
    order = []
    for p in range(3):
        for w in range(2):
            order += [("D", w, k, p) for k in (ts if p else ks)]
    order += [("F", 0, k) for k in ks] + [("S", 0)] + [("C", 0, k, 0) for k in ks]
    order += [("F", 1, k) for k in ks] + [("S", 1)] + [("C", 1, k, 0) for k in ks]
    for p in range(1, 3):
        for w in range(2):
            order += [("C", w, t, p) for t in ts]
    return order + [("E", w, k) for w in range(2) for k in ks]


def layer_kernel(
    ci_h, gi_h, go_h, taps_h, docs_h, res_h, op_h, gain_h, ids_h, wts_h, wg_h, wu_h, wd_h,
    out,
    ci, gi, go, taps, docs, ids, wts, gain, res, opv, wg, wu, wd,
    inner, halo_send, halo_all, fix_send, fix_all, docs8, conv_send, conv_all,
    carried, meta_send, meta, tok, pack, there, gsum, usum, hid, back, comb,
    part_send, part_recv,
    load_sem, halo_s, halo_r, fix_s, fix_r, meta_s, meta_r, tp_send, tp_recv, tok_send, tok_recv,
    d_send, d_recv, c_send, c_recv, p_send, p_recv,
):
    sp = lax.axis_index("sp")
    x = lax.axis_index("tp")
    c = sp % 2
    y = (sp // 2) % 4
    z = sp // 8
    here = [z, y, x]

    def along(axis, step):
        at = [z, y, x]
        at[axis] = (at[axis] + step) % 4
        return ((at[0] * 4 + at[1]) * 2 + c, at[2])

    twin = (sp + 1 - 2 * c, x)
    after = ((sp + 1) % 32, 0)
    tp_far = [(sp, (x + j) % 4) for j in range(4)]

    def load(src, dst, i):
        return pltpu.make_async_copy(src, dst, load_sem.at[i])

    pairs = [(ci_h, ci), (gi_h, gi), (taps_h, taps), (docs_h, docs), (ids_h, ids), (wts_h, wts), (go_h, go),
             (gain_h, gain), (res_h, res), (op_h, opv), (wg_h.at[0], wg), (wu_h.at[0], wu), (wd_h.at[0], wd)]
    loads = [load(src, dst, i) for i, (src, dst) in enumerate(pairs)]
    for i in range(7):
        loads[i].start()

    bar = pltpu.get_barrier_semaphore()
    for axis in range(3):
        for step in STEPS:
            pl.semaphore_signal(bar, inc=1, device_id=along(axis, step), device_id_type=MESH)
    pl.semaphore_signal(bar, inc=1, device_id=twin, device_id_type=MESH)

    @pl.when(x == 0)
    def _():
        for t in range(4):
            pl.semaphore_signal(bar, inc=1, device_id=((sp + 31) % 32, t), device_id_type=MESH)

    for i in range(6):
        loads[i].wait()
    for i in range(7, 13):
        loads[i].start()
    meta_send[0:2, :] = ids[...].astype(F32)
    meta_send[2:4, :] = wts[...]
    docs8[0:1, :] = jnp.full((1, 128), -1, jnp.int32)
    docs8[1:5, :] = docs[...]
    inner[0:8, :] = jnp.zeros((8, 256), F32)
    inner[8:520, :] = ci[...].astype(F32) * gi[...].astype(F32)

    def remote(src, dst, ssem, rsem, dev):
        return pltpu.make_async_remote_copy(
            src_ref=src, dst_ref=dst, send_sem=ssem, recv_sem=rsem, device_id=dev, device_id_type=MESH
        )

    t0 = taps[0:1, :].astype(F32)
    t1 = taps[1:2, :].astype(F32)
    t2 = taps[2:3, :].astype(F32)
    last = docs[3:4, :].astype(F32)
    halo_send[0:1, :] = t1 * inner[519:520, :]
    halo_send[1:2, :] = t0 * inner[518:519, :]
    halo_send[2:3, :] = t0 * inner[519:520, :]
    halo_send[3:4, :] = jnp.broadcast_to(last[:, 127:128], (1, 256))
    halo_send[4:5, :] = jnp.broadcast_to(last[:, 126:127], (1, 256))

    pl.semaphore_wait(bar, 11)
    halo_copy = remote(halo_send, halo_all.at[x], halo_s, halo_r.at[x], after)
    meta_copy = remote(meta_send, meta, meta_s, meta_r, twin)
    halo_copy.start()
    meta_copy.start()

    rows = lax.broadcasted_iota(jnp.int32, (128, 128), 0)
    lanes = lax.broadcasted_iota(jnp.int32, (128, 128), 1)
    eye = jnp.where(rows == lanes, 1.0, 0.0).astype(F32)

    def column(row):
        return jnp.sum(eye * row, axis=1, keepdims=True)

    lane8 = lax.broadcasted_iota(jnp.int32, (8, 128), 1)

    def conv_block(b):
        cur = jnp.broadcast_to(docs8[b + 1 : b + 2, :], (8, 128))
        prev = jnp.broadcast_to(docs8[b : b + 1, :], (8, 128))
        one = jnp.where(lane8 < 1, pltpu.roll(prev, 1, 1), pltpu.roll(cur, 1, 1))
        two = jnp.where(lane8 < 2, pltpu.roll(prev, 2, 1), pltpu.roll(cur, 2, 1))
        m1 = column(jnp.where(one == cur, 1.0, 0.0).astype(F32)[0:1, :])
        m2 = column(jnp.where(two == cur, 1.0, 0.0).astype(F32)[0:1, :])
        base = 8 + 128 * b
        i0 = inner[base : base + 128, :]
        i1 = inner[base - 1 : base + 127, :]
        i2 = inner[base - 2 : base + 126, :]
        value = t2 * i0 + t1 * (m1 * i1) + t0 * (m2 * i2)
        gate = go[128 * b : 128 * b + 128, :].astype(F32)
        conv_send[b] = (gate * value).astype(BF)
        if b == 0:
            fix_send[0:8, :] = value[0:8, :]
            fix_send[8:16, :] = gate[0:8, :]

    def tp_copy(b):
        slot = (b + 4 - x) % 4
        return remote(conv_send.at[b], conv_all.at[x], tp_send.at[slot], tp_recv.at[slot], (sp, b))

    def fix_copy(t):
        return remote(fix_send, fix_all.at[t], fix_s, fix_r.at[t], (sp, 0))

    loads[6].wait()
    for b in range(4):
        conv_block(b)

        @pl.when(x != b)
        def _():
            tp_copy(b).start()
            if b == 0:
                fix_copy(x).start()

        @pl.when(x == b)
        def _():
            conv_all[b] = conv_send[b]
            if b == 0:
                fix_all[0] = fix_send[...]

    meta_copy.wait_recv()

    def routing(table):
        e = [table[a : a + 1, :] for a in range(2)]
        ec = [column(v) for v in e]
        out_rows = []
        for a in range(2):
            same = ((ec[0] == e[a]) | (ec[1] == e[a])) & (rows < lanes)
            rank = jnp.sum(jnp.where(same, 1.0, 0.0).astype(F32), axis=0, keepdims=True)
            ei = e[a].astype(jnp.int32)

            ahead = (((ei >> 5) & 3) - z + 4) & 3
            unit = (ei & 3) + 4 * ((ei >> 3) & 3) + 16 * (2 * (ahead & 1) + (ahead >> 1))
            out_rows.append((unit * 8 + rank.astype(jnp.int32), (ei >> 2) & 1))
        return out_rows

    slot_rows = lax.broadcasted_iota(jnp.int32, (512, 128), 0)
    slot_lanes = lax.broadcasted_iota(jnp.int32, (128, 512), 1).astype(F32)
    for s, table in ((0, meta_send), (1, meta)):
        source_core = c if s == 0 else 1 - c
        targets = []
        for slot, parity in routing(table):
            targets.append(jnp.where(parity == c, slot + 4 * source_core, -1))
        hit = (slot_rows == targets[0]) | (slot_rows == targets[1])
        pack[:, 128 * s : 128 * s + 128] = jnp.where(hit, 1.0, 0.0).astype(F32).astype(BF)
        weight = jnp.zeros((128, 512), F32)
        for a in range(2):
            tc = column(targets[a].astype(F32))
            wc = column(table[2 + a : 3 + a, :])
            weight = weight + jnp.where(slot_lanes == tc, wc, 0.0)
        high = weight.astype(BF)
        comb[0, 128 * s : 128 * s + 128, :] = high
        comb[1, 128 * s : 128 * s + 128, :] = (weight - high.astype(F32)).astype(BF)

    for i in (7, 8, 9):
        loads[i].wait()
    for j in range(1, 4):
        pltpu.make_async_remote_copy(
            src_ref=conv_send.at[0], dst_ref=conv_all.at[(x + 4 - j) % 4], send_sem=tp_send.at[j],
            recv_sem=tp_recv.at[j], device_id=tp_far[j], device_id_type=MESH,
        ).wait_recv()

    @pl.when(x == 0)
    def _():
        edge = lax.broadcasted_iota(jnp.int32, (8, 256), 0)
        first = docs[0:1, :].astype(F32)
        inside = jnp.where(sp == 0, 0.0, 1.0)
        for t in range(4):
            if t > 0:
                fix_copy(t).wait_recv()
            remote(halo_send, halo_all.at[t], halo_s, halo_r.at[t], after).wait_recv()
            from_behind = halo_all[t]
            m1 = jnp.where(from_behind[3:4] == first[:, 0:1], inside, 0.0)
            m2 = jnp.where(from_behind[4:5] == first[:, 0:1], inside, 0.0)
            m3 = jnp.where(from_behind[3:4] == first[:, 1:2], inside, 0.0)
            add0 = m1 * from_behind[0:1] + m2 * from_behind[1:2]
            add1 = m3 * from_behind[2:3]
            extra = jnp.where(edge == 0, add0, jnp.where(edge == 1, add1, 0.0))
            fixed = fix_all[t, 8:16, :] * (fix_all[t, 0:8, :] + extra)
            conv_all[t, 0:8, :] = fixed.astype(BF)

    total = jnp.zeros((128, 1), F32)
    for n in range(NCH):
        cols = slice(W * n, W * n + W)
        acc = jnp.zeros((128, W), F32)
        for i in range(4):
            acc = acc + jnp.dot(conv_all[i], opv[256 * i : 256 * i + 256, cols], preferred_element_type=F32)
        value = res[:, cols].astype(F32) + acc.astype(BF).astype(F32)
        total = total + jnp.sum(value * value, axis=1, keepdims=True)
        carried[n] = value
    scale = lax.rsqrt(total / 2048.0 + 1e-6)

    def tok_copy(j):
        ks = pl.ds(TOKS * j, TOKS)
        return remote(tok.at[ks, pl.ds(0, 128)], tok.at[ks, pl.ds(128, 128)], tok_send.at[j], tok_recv.at[j], twin)

    for k in range(NCH):
        tok[k, 0:128, :] = (carried[k] * scale * gain[:, W * k : W * k + W]).astype(BF)
        if (k + 1) % TOKS == 0:
            tok_copy(k // TOKS).start()

    def plane(buf, w, p, k, axis, v):
        index = [slice(None)] * 3
        index[axis] = v
        return buf.at[(w, p, k, *index)]

    def axis_of(w, p, k):
        return (k + p + w) % 3

    def moves(buf, ss, rs, w, p, k, sign):
        axis = axis_of(w, p, k)
        found = []
        if axis == 0:
            for j in range(2):
                step = (w + 2 * j) * sign % 4
                if step != 0:
                    found.append((plane(buf, w, p, k, 0, j), plane(buf, w, p + 1, k, 0, j), step))
        else:
            for step in STEPS:
                source = plane(buf, w, p, k, axis, (here[axis] + step) % 4)
                found.append((source, plane(buf, w, p + 1, k, axis, here[axis]), step))
        return [
            remote(src, dst, ss.at[w, p, k, n], rs.at[w, p, k, n], along(axis, step))
            for n, (src, dst, step) in enumerate(found)
        ]

    def begin(buf, ss, rs, w, p, k, sign):
        for copy in moves(buf, ss, rs, w, p, k, sign):
            copy.start()
        axis = axis_of(w, p, k)
        if axis != 0:
            stay = plane(buf, w, p + 1, k, axis, here[axis])
            stay[...] = plane(buf, w, p, k, axis, here[axis])[...]
        elif w == 0:
            stay = plane(buf, w, p + 1, k, 0, 0)
            stay[...] = plane(buf, w, p, k, 0, 0)[...]

    def settle(buf, ss, rs, w, p, k, sign):
        for copy in moves(buf, ss, rs, w, p, k, sign):
            copy.wait_recv()

    out_way = (there, d_send, d_recv)
    home_way = (back, c_send, c_recv)

    def pieces(k):
        return range(PARTS * k, PARTS * k + PARTS)

    def put(buf, w, k, value):
        for i, t in enumerate(pieces(k)):
            buf[w, 0, t] = value[:, PW * i : PW * i + PW].reshape(CUBE).astype(BF)

    def rows_of(buf, w, k):
        parts = [buf[w, 3, t].astype(F32).reshape(HALF, PW).astype(BF) for t in pieces(k)]
        return jnp.concatenate(parts, axis=1)

    def step_out(w, k, p):
        if p == 0:
            if w == 0 and k % TOKS == 0:
                tok_copy(k // TOKS).wait_recv()
            packed = jnp.dot(pack[HALF * w : HALF * w + HALF, :], tok[k], preferred_element_type=F32)
            put(there, w, k, packed)
            for t in pieces(k):
                begin(*out_way, w, p, t, 1)
        else:
            settle(*out_way, w, p - 1, k, 1)
            begin(*out_way, w, p, k, 1)

    def gate_up(w, k):
        if w == 0 and k == 0:
            loads[10].wait()
            loads[11].wait()
        for t in pieces(k):
            settle(*out_way, w, 2, t, 1)
        source = rows_of(there, w, k)
        rows_k = slice(W * k, W * k + W)
        g = jnp.dot(source, wg[rows_k, :], preferred_element_type=F32)
        u = jnp.dot(source, wu[rows_k, :], preferred_element_type=F32)
        if k == 0:
            gsum[w] = g
            usum[w] = u
        else:
            gsum[w] += g
            usum[w] += u

    def activate(w):
        @pl.loop(0, 8)
        def _(r):
            rs = pl.ds(pl.multiple_of(r * 32, 32), 32)
            half = 0.5 * gsum[w, rs, :]
            hid[w, rs, :] = ((half + half * jnp.tanh(half)) * usum[w, rs, :]).astype(BF)

        if w == 0:
            loads[12].wait()

    def step_home(w, k, p):
        if p == 0:
            put(back, w, k, jnp.dot(hid[w], wd[:, W * k : W * k + W], preferred_element_type=F32))
            for t in pieces(k):
                begin(*home_way, w, p, t, -1)
        else:
            settle(*home_way, w, p - 1, k, -1)
            begin(*home_way, w, p, k, -1)

    def part_copy(k):
        return remote(part_send.at[k], part_recv.at[k], p_send.at[k], p_recv.at[k], twin)

    def collect(w, k):
        for t in pieces(k):
            settle(*home_way, w, 2, t, -1)
        source = rows_of(back, w, k)
        slots = slice(HALF * w, HALF * w + HALF)
        both = jnp.dot(comb[0, :, slots], source, preferred_element_type=F32) + jnp.dot(
            comb[1, :, slots], source, preferred_element_type=F32
        )
        carried[k] += both[:128]
        if w == 0:
            part_send[k] = both[128:]
        else:
            part_send[k] += both[128:]
            part_copy(k).start()

    actions = {"D": step_out, "F": gate_up, "S": activate, "C": step_home, "E": collect}
    for name, *where in schedule():
        actions[name](*where)

    for k in range(NCH):
        part_copy(k).wait_recv()
        out[:, W * k : W * k + W] = (carried[k] + part_recv[k]).astype(BF)

    halo_copy.wait_send()
    meta_copy.wait_send()

    @pl.when(x != 0)
    def _():
        fix_copy(x).wait_send()

    for w in range(2):
        for p in range(3):
            for k in range(PIECES):
                for copy in moves(*out_way, w, p, k, 1) + moves(*home_way, w, p, k, -1):
                    copy.wait_send()
    for j in range(1, 4):
        pltpu.make_async_remote_copy(
            src_ref=conv_send.at[0], dst_ref=conv_all.at[0], send_sem=tp_send.at[j],
            recv_sem=tp_recv.at[j], device_id=tp_far[j], device_id_type=MESH,
        ).wait_send()
    for j in range(NCH // TOKS):
        tok_copy(j).wait_send()
    for k in range(NCH):
        part_copy(k).wait_send()


def on_device(ci, gi, go, taps, docs, res, op, gain, ids, wts, wg, wu, wd):
    vmem = pl.BlockSpec(memory_space=pltpu.VMEM)
    hbm = pl.BlockSpec(memory_space=pltpu.HBM)
    dma = pltpu.SemaphoreType.DMA
    scratch = [
        pltpu.VMEM((512, 256), BF), pltpu.VMEM((512, 256), BF), pltpu.VMEM((512, 256), BF),
        pltpu.VMEM((3, 256), BF), pltpu.VMEM((4, 128), jnp.int32), pltpu.VMEM((2, 128), jnp.int32),
        pltpu.VMEM((2, 128), F32), pltpu.VMEM((1, 2048), F32),
        pltpu.VMEM((128, 2048), BF), pltpu.VMEM((1024, 2048), BF),
        pltpu.VMEM((2048, 1024), BF), pltpu.VMEM((2048, 1024), BF), pltpu.VMEM((1024, 2048), BF),
        pltpu.VMEM((520, 256), F32), pltpu.VMEM((8, 256), F32), pltpu.VMEM((4, 8, 256), F32),
        pltpu.VMEM((16, 256), F32), pltpu.VMEM((4, 16, 256), F32),
        pltpu.VMEM((8, 128), jnp.int32), pltpu.VMEM((4, 128, 256), BF), pltpu.VMEM((4, 128, 256), BF),
        pltpu.VMEM((NCH, 128, W), F32), pltpu.VMEM((4, 128), F32), pltpu.VMEM((4, 128), F32),
        pltpu.VMEM((NCH, 256, W), BF), pltpu.VMEM((512, 256), BF), pltpu.VMEM((2, 4, PIECES, *CUBE), BF),
        pltpu.VMEM((2, HALF, 1024), F32), pltpu.VMEM((2, HALF, 1024), F32), pltpu.VMEM((2, HALF, 1024), BF),
        pltpu.VMEM((2, 4, PIECES, *CUBE), BF), pltpu.VMEM((2, 256, 512), BF),
        pltpu.VMEM((NCH, 128, W), F32), pltpu.VMEM((NCH, 128, W), F32),
        dma((13,)), dma, dma((4,)), dma, dma((4,)), dma, dma, dma((4,)), dma((4,)), dma((NCH,)), dma((NCH,)),
        dma((2, 3, PIECES, 3)), dma((2, 3, PIECES, 3)), dma((2, 3, PIECES, 3)), dma((2, 3, PIECES, 3)), dma((NCH,)), dma((NCH,)),
    ]
    arrays = (ci, gi, go, taps, docs.reshape(4, 128), res, op, gain.reshape(1, 2048), ids.T, wts.T, wg, wu, wd)
    arrays = [pltpu.with_memory_space_constraint(v, pltpu.HBM) for v in arrays]
    return pl.pallas_call(
        layer_kernel,
        out_shape=jax.ShapeDtypeStruct((128, 2048), BF),
        in_specs=[hbm] * 13,
        out_specs=vmem,
        scratch_shapes=scratch,
        compiler_params=pltpu.CompilerParams(
            collective_id=0, has_side_effects=True, vmem_limit_bytes=54000000
        ),
    )(*arrays)


def solution(mesh):
    in_specs = (
        P("sp", "tp"),
        P("sp", "tp"),
        P("sp", "tp"),
        P(None, "tp"),
        P("sp"),
        P(("sp", "tp"), None),
        P(),
        P(),
        P(("sp", "tp"), None),
        P(("sp", "tp"), None),
        P(("sp", "tp"), None, None),
        P(("sp", "tp"), None, None),
        P(("sp", "tp"), None, None),
    )
    out_specs = P(("sp", "tp"), None)
    return jax.shard_map(
        on_device, mesh=mesh, in_specs=in_specs, out_specs=out_specs, check_vma=False
    )
```

```python
import jax
import jax.numpy as jnp
from jax import lax
from jax.experimental import pallas as pl
from jax.experimental.pallas import tpu as pltpu
from jax.sharding import PartitionSpec as P

MESH = pl.DeviceIdType.MESH
BF = jnp.bfloat16
F32 = jnp.float32
WIDTHS = (512, 512, 512, 512)
STARTS = (0, 512, 1024, 1536)
NCH = len(WIDTHS)
WIDE = max(WIDTHS)
CUBE = (2, 4, 4, 8, WIDE)
HALF = 256
STEPS = (1, 3, 2)


def schedule():
    ks = range(NCH)
    order = []
    for p in range(3):
        for w in range(2):
            order += [("D", w, k, p) for k in ks]
    order += [("F", 0, k) for k in ks] + [("C", 0, k, 0) for k in ks]
    order += [("F", 1, k) for k in ks] + [("C", 1, k, 0) for k in ks]
    for p in range(1, 3):
        for w in range(2):
            order += [("C", w, k, p) for k in ks]
    return order + [("E", w, k) for w in range(2) for k in ks]


def layer_kernel(
    ci_h, gi_h, go_h, taps_h, docs_h, res_h, op_h, gain_h, ids_h, wts_h, wg_h, wu_h, wd_h,
    out,
    ci, gi, go, taps, docs, ids, wts, gain, res, opv, wg, wu, wd,
    inner, halo_send, halo_all, fix_send, fix_all, docs8, conv_send, conv_all,
    carried, meta_send, meta, tok, pack, there, gsum, usum, hid, back, comb,
    part_send, part_recv,
    load_sem, halo_s, halo_r, fix_s, fix_r, meta_s, meta_r, tp_send, tp_recv, tok_send, tok_recv,
    d_send, d_recv, c_send, c_recv, p_send, p_recv,
):
    sp = lax.axis_index("sp")
    x = lax.axis_index("tp")
    c = sp % 2
    y = (sp // 2) % 4
    z = sp // 8
    here = [z, y + c * (x - y), x + c * (y - x)]

    def along(axis, step):
        at = list(here)
        at[axis] = (at[axis] + step) % 4
        row, col = at[1] + c * (at[2] - at[1]), at[2] + c * (at[1] - at[2])
        return ((at[0] * 4 + row) * 2 + c, col)

    twin = (sp + 1 - 2 * c, x)
    after = ((sp + 1) % 32, 0)
    tp_far = [(sp, (x + j) % 4) for j in range(4)]

    def load(src, dst, i):
        return pltpu.make_async_copy(src, dst, load_sem.at[i])

    pairs = [(ci_h, ci), (gi_h, gi), (taps_h, taps), (docs_h, docs), (ids_h, ids), (wts_h, wts), (go_h, go),
             (gain_h, gain), (res_h, res), (op_h, opv), (wg_h.at[0], wg), (wu_h.at[0], wu), (wd_h.at[0], wd)]
    loads = [load(src, dst, i) for i, (src, dst) in enumerate(pairs)]
    for i in range(7):
        loads[i].start()

    bar = pltpu.get_barrier_semaphore()
    for axis in range(3):
        for step in STEPS:
            pl.semaphore_signal(bar, inc=1, device_id=along(axis, step), device_id_type=MESH)
    pl.semaphore_signal(bar, inc=1, device_id=twin, device_id_type=MESH)

    @pl.when(x == 0)
    def _():
        for t in range(4):
            pl.semaphore_signal(bar, inc=1, device_id=((sp + 31) % 32, t), device_id_type=MESH)

    for i in range(6):
        loads[i].wait()
    for i in range(7, 13):
        loads[i].start()
    meta_send[0:2, :] = ids[...].astype(F32)
    meta_send[2:4, :] = wts[...]
    docs8[0:1, :] = jnp.full((1, 128), -1, jnp.int32)
    docs8[1:5, :] = docs[...]
    inner[0:8, :] = jnp.zeros((8, 256), F32)
    inner[8:520, :] = ci[...].astype(F32) * gi[...].astype(F32)

    def remote(src, dst, ssem, rsem, dev):
        return pltpu.make_async_remote_copy(
            src_ref=src, dst_ref=dst, send_sem=ssem, recv_sem=rsem, device_id=dev, device_id_type=MESH
        )

    t0 = taps[0:1, :].astype(F32)
    t1 = taps[1:2, :].astype(F32)
    t2 = taps[2:3, :].astype(F32)
    last = docs[3:4, :].astype(F32)
    halo_send[0:1, :] = t1 * inner[519:520, :]
    halo_send[1:2, :] = t0 * inner[518:519, :]
    halo_send[2:3, :] = t0 * inner[519:520, :]
    halo_send[3:4, :] = jnp.broadcast_to(last[:, 127:128], (1, 256))
    halo_send[4:5, :] = jnp.broadcast_to(last[:, 126:127], (1, 256))

    pl.semaphore_wait(bar, 11)
    halo_copy = remote(halo_send, halo_all.at[x], halo_s, halo_r.at[x], after)
    meta_copy = remote(meta_send, meta, meta_s, meta_r, twin)
    halo_copy.start()
    meta_copy.start()

    rows = lax.broadcasted_iota(jnp.int32, (128, 128), 0)
    lanes = lax.broadcasted_iota(jnp.int32, (128, 128), 1)
    eye = jnp.where(rows == lanes, 1.0, 0.0).astype(F32)

    def column(row):
        return jnp.sum(eye * row, axis=1, keepdims=True)

    lane8 = lax.broadcasted_iota(jnp.int32, (8, 128), 1)

    def conv_block(b):
        cur = jnp.broadcast_to(docs8[b + 1 : b + 2, :], (8, 128))
        prev = jnp.broadcast_to(docs8[b : b + 1, :], (8, 128))
        one = jnp.where(lane8 < 1, pltpu.roll(prev, 1, 1), pltpu.roll(cur, 1, 1))
        two = jnp.where(lane8 < 2, pltpu.roll(prev, 2, 1), pltpu.roll(cur, 2, 1))
        m1 = column(jnp.where(one == cur, 1.0, 0.0).astype(F32)[0:1, :])
        m2 = column(jnp.where(two == cur, 1.0, 0.0).astype(F32)[0:1, :])
        base = 8 + 128 * b
        i0 = inner[base : base + 128, :]
        i1 = inner[base - 1 : base + 127, :]
        i2 = inner[base - 2 : base + 126, :]
        value = t2 * i0 + t1 * (m1 * i1) + t0 * (m2 * i2)
        gate = go[128 * b : 128 * b + 128, :].astype(F32)
        conv_send[b] = (gate * value).astype(BF)
        if b == 0:
            fix_send[0:8, :] = value[0:8, :]
            fix_send[8:16, :] = gate[0:8, :]

    def tp_copy(j):
        return remote(conv_send.at[(x + j) % 4], conv_all.at[x], tp_send.at[j], tp_recv.at[j], tp_far[j])

    def fix_copy(t):
        return remote(fix_send, fix_all.at[t], fix_s, fix_r.at[t], (sp, 0))

    loads[6].wait()
    for b in range(4):
        conv_block(b)

    @pl.when(x != 0)
    def _():
        fix_copy(x).start()

    for j in STEPS:
        tp_copy(j).start()
    conv_all[x] = conv_send[x]

    @pl.when(x == 0)
    def _():
        fix_all[0] = fix_send[...]

    meta_copy.wait_recv()

    def routing(table):
        e = [table[a : a + 1, :] for a in range(2)]
        ec = [column(v) for v in e]
        out_rows = []
        for a in range(2):
            same = ((ec[0] == e[a]) | (ec[1] == e[a])) & (rows < lanes)
            rank = jnp.sum(jnp.where(same, 1.0, 0.0).astype(F32), axis=0, keepdims=True)
            ei = e[a].astype(jnp.int32)

            ahead = (((ei >> 5) & 3) - z + 4) & 3
            row, col = (ei >> 3) & 3, ei & 3
            unit = col + c * (row - col) + 4 * (row + c * (col - row)) + 16 * (2 * (ahead & 1) + (ahead >> 1))
            out_rows.append((unit * 8 + rank.astype(jnp.int32), (ei >> 2) & 1))
        return out_rows

    slot_rows = lax.broadcasted_iota(jnp.int32, (512, 128), 0)
    slot_lanes = lax.broadcasted_iota(jnp.int32, (128, 512), 1).astype(F32)
    for s, table in ((0, meta_send), (1, meta)):
        source_core = c if s == 0 else 1 - c
        targets = []
        for slot, parity in routing(table):
            targets.append(jnp.where(parity == c, slot + 4 * source_core, -1))
        hit = (slot_rows == targets[0]) | (slot_rows == targets[1])
        pack[:, 128 * s : 128 * s + 128] = jnp.where(hit, 1.0, 0.0).astype(F32).astype(BF)
        weight = jnp.zeros((128, 512), F32)
        for a in range(2):
            tc = column(targets[a].astype(F32))
            wc = column(table[2 + a : 3 + a, :])
            weight = weight + jnp.where(slot_lanes == tc, wc, 0.0)
        high = weight.astype(BF)
        comb[0, 128 * s : 128 * s + 128, :] = high
        comb[1, 128 * s : 128 * s + 128, :] = (weight - high.astype(F32)).astype(BF)

    for i in (7, 8, 9):
        loads[i].wait()
    for j in range(1, 4):
        pltpu.make_async_remote_copy(
            src_ref=conv_send.at[0], dst_ref=conv_all.at[(x + 4 - j) % 4], send_sem=tp_send.at[j],
            recv_sem=tp_recv.at[j], device_id=tp_far[j], device_id_type=MESH,
        ).wait_recv()

    @pl.when(x == 0)
    def _():
        edge = lax.broadcasted_iota(jnp.int32, (8, 256), 0)
        first = docs[0:1, :].astype(F32)
        inside = jnp.where(sp == 0, 0.0, 1.0)
        for t in range(4):
            if t > 0:
                fix_copy(t).wait_recv()
            remote(halo_send, halo_all.at[t], halo_s, halo_r.at[t], after).wait_recv()
            from_behind = halo_all[t]
            m1 = jnp.where(from_behind[3:4] == first[:, 0:1], inside, 0.0)
            m2 = jnp.where(from_behind[4:5] == first[:, 0:1], inside, 0.0)
            m3 = jnp.where(from_behind[3:4] == first[:, 1:2], inside, 0.0)
            add0 = m1 * from_behind[0:1] + m2 * from_behind[1:2]
            add1 = m3 * from_behind[2:3]
            extra = jnp.where(edge == 0, add0, jnp.where(edge == 1, add1, 0.0))
            fixed = fix_all[t, 8:16, :] * (fix_all[t, 0:8, :] + extra)
            conv_all[t, 0:8, :] = fixed.astype(BF)

    total = jnp.zeros((128, 1), F32)
    for k in range(NCH):
        for n in range(0, WIDTHS[k], 256):
            cols = slice(STARTS[k] + n, STARTS[k] + n + 256)
            acc = jnp.zeros((128, 256), F32)
            for i in range(4):
                acc = acc + jnp.dot(conv_all[i], opv[256 * i : 256 * i + 256, cols], preferred_element_type=F32)
            value = res[:, cols].astype(F32) + acc.astype(BF).astype(F32)
            total = total + jnp.sum(value * value, axis=1, keepdims=True)
            carried[k, :, n : n + 256] = value
    scale = lax.rsqrt(total / 2048.0 + 1e-6)

    def tok_copy(k):
        lanes_k = pl.ds(0, WIDTHS[k])
        return remote(
            tok.at[k, pl.ds(0, 128), lanes_k], tok.at[k, pl.ds(128, 128), lanes_k],
            tok_send.at[k], tok_recv.at[k], twin,
        )

    for k in range(NCH):
        width, start = WIDTHS[k], STARTS[k]
        normed = carried[k, :, :width] * scale * gain[:, start : start + width]
        tok[k, 0:128, :width] = normed.astype(BF)
        tok_copy(k).start()

    def plane(buf, w, p, k, axis, v):
        index = [slice(None)] * 3
        index[axis] = v
        return buf.at[(w, p, k, *index, slice(None), pl.ds(0, WIDTHS[k]))]

    def axis_of(w, p, k):
        return (k + 2 * p + w) % 3

    def moves(buf, ss, rs, w, p, k, sign):
        axis = axis_of(w, p, k)
        found = []
        if axis == 0:
            for j in range(2):
                step = (w + 2 * j) * sign % 4
                if step != 0:
                    found.append((plane(buf, w, p, k, 0, j), plane(buf, w, p + 1, k, 0, j), step))
        else:
            for step in STEPS:
                source = plane(buf, w, p, k, axis, (here[axis] + step) % 4)
                found.append((source, plane(buf, w, p + 1, k, axis, here[axis]), step))
        return [
            remote(src, dst, ss.at[w, p, k, n], rs.at[w, p, k, n], along(axis, step))
            for n, (src, dst, step) in enumerate(found)
        ]

    def begin(buf, ss, rs, w, p, k, sign):
        for copy in moves(buf, ss, rs, w, p, k, sign):
            copy.start()
        axis = axis_of(w, p, k)
        if axis != 0:
            stay = plane(buf, w, p + 1, k, axis, here[axis])
            stay[...] = plane(buf, w, p, k, axis, here[axis])[...]
        elif w == 0:
            stay = plane(buf, w, p + 1, k, 0, 0)
            stay[...] = plane(buf, w, p, k, 0, 0)[...]

    def settle(buf, ss, rs, w, p, k, sign):
        for copy in moves(buf, ss, rs, w, p, k, sign):
            copy.wait_recv()

    out_way = (there, d_send, d_recv)
    home_way = (back, c_send, c_recv)

    def columns(k):
        return slice(STARTS[k], STARTS[k] + WIDTHS[k])

    def put(buf, w, k, value):
        buf[w, 0, k, :, :, :, :, : WIDTHS[k]] = value.reshape(*CUBE[:4], WIDTHS[k]).astype(BF)

    def rows_of(buf, w, k):
        return buf[w, 3, k, :, :, :, :, : WIDTHS[k]].astype(F32).reshape(HALF, WIDTHS[k]).astype(BF)

    def step_out(w, k, p):
        if p == 0:
            if w == 0:
                tok_copy(k).wait_recv()
            source = tok[k, :, : WIDTHS[k]]
            put(there, w, k, jnp.dot(pack[HALF * w : HALF * w + HALF, :], source, preferred_element_type=F32))
        else:
            settle(*out_way, w, p - 1, k, 1)
        begin(*out_way, w, p, k, 1)

    def gate_up(w, k):
        if w == 0 and k == 0:
            loads[10].wait()
            loads[11].wait()
        settle(*out_way, w, 2, k, 1)
        source = rows_of(there, w, k)
        rows_k = columns(k)
        if k == NCH - 1:
            for n in range(0, 1024, 256):
                block = slice(n, n + 256)
                g = gsum[w, :, block] + jnp.dot(source, wg[rows_k, block], preferred_element_type=F32)
                u = usum[w, :, block] + jnp.dot(source, wu[rows_k, block], preferred_element_type=F32)
                half = 0.5 * g
                hid[w, :, block] = ((half + half * jnp.tanh(half)) * u).astype(BF)
            return
        g = jnp.dot(source, wg[rows_k, :], preferred_element_type=F32)
        u = jnp.dot(source, wu[rows_k, :], preferred_element_type=F32)
        if k == 0:
            gsum[w] = g
            usum[w] = u
        else:
            gsum[w] += g
            usum[w] += u

    def step_home(w, k, p):
        if w == 0 and k == 0 and p == 0:
            loads[12].wait()
        if p == 0:
            put(back, w, k, jnp.dot(hid[w], wd[:, columns(k)], preferred_element_type=F32))
        else:
            settle(*home_way, w, p - 1, k, -1)
        begin(*home_way, w, p, k, -1)

    def part_copy(k):
        part = (k, slice(None), pl.ds(0, WIDTHS[k]))
        return remote(part_send.at[part], part_recv.at[part], p_send.at[k], p_recv.at[k], twin)

    def collect(w, k):
        settle(*home_way, w, 2, k, -1)
        source = rows_of(back, w, k)
        slots = slice(HALF * w, HALF * w + HALF)
        both = jnp.dot(comb[0, :, slots], source, preferred_element_type=F32) + jnp.dot(
            comb[1, :, slots], source, preferred_element_type=F32
        )
        carried[k, :, : WIDTHS[k]] += both[:128]
        if w == 0:
            part_send[k, :, : WIDTHS[k]] = both[128:]
        else:
            part_send[k, :, : WIDTHS[k]] += both[128:]
            part_copy(k).start()

    actions = {"D": step_out, "F": gate_up, "C": step_home, "E": collect}
    for name, *where in schedule():
        actions[name](*where)

    for k in range(NCH):
        part_copy(k).wait_recv()
        width = WIDTHS[k]
        out[:, columns(k)] = (carried[k, :, :width] + part_recv[k, :, :width]).astype(BF)

    halo_copy.wait_send()
    meta_copy.wait_send()

    @pl.when(x != 0)
    def _():
        fix_copy(x).wait_send()

    for w in range(2):
        for p in range(3):
            for k in range(NCH):
                for copy in moves(*out_way, w, p, k, 1) + moves(*home_way, w, p, k, -1):
                    copy.wait_send()
    for j in range(1, 4):
        pltpu.make_async_remote_copy(
            src_ref=conv_send.at[0], dst_ref=conv_all.at[0], send_sem=tp_send.at[j],
            recv_sem=tp_recv.at[j], device_id=tp_far[j], device_id_type=MESH,
        ).wait_send()
    for j in range(NCH):
        tok_copy(j).wait_send()
    for k in range(NCH):
        part_copy(k).wait_send()


def on_device(ci, gi, go, taps, docs, res, op, gain, ids, wts, wg, wu, wd):
    vmem = pl.BlockSpec(memory_space=pltpu.VMEM)
    hbm = pl.BlockSpec(memory_space=pltpu.HBM)
    dma = pltpu.SemaphoreType.DMA
    scratch = [
        pltpu.VMEM((512, 256), BF), pltpu.VMEM((512, 256), BF), pltpu.VMEM((512, 256), BF),
        pltpu.VMEM((3, 256), BF), pltpu.VMEM((4, 128), jnp.int32), pltpu.VMEM((2, 128), jnp.int32),
        pltpu.VMEM((2, 128), F32), pltpu.VMEM((1, 2048), F32),
        pltpu.VMEM((128, 2048), BF), pltpu.VMEM((1024, 2048), BF),
        pltpu.VMEM((2048, 1024), BF), pltpu.VMEM((2048, 1024), BF), pltpu.VMEM((1024, 2048), BF),
        pltpu.VMEM((520, 256), F32), pltpu.VMEM((8, 256), F32), pltpu.VMEM((4, 8, 256), F32),
        pltpu.VMEM((16, 256), F32), pltpu.VMEM((4, 16, 256), F32),
        pltpu.VMEM((8, 128), jnp.int32), pltpu.VMEM((4, 128, 256), BF), pltpu.VMEM((4, 128, 256), BF),
        pltpu.VMEM((NCH, 128, WIDE), F32), pltpu.VMEM((4, 128), F32), pltpu.VMEM((4, 128), F32),
        pltpu.VMEM((NCH, 256, WIDE), BF), pltpu.VMEM((512, 256), BF), pltpu.VMEM((2, 4, NCH, *CUBE), BF),
        pltpu.VMEM((2, HALF, 1024), F32), pltpu.VMEM((2, HALF, 1024), F32), pltpu.VMEM((2, HALF, 1024), BF),
        pltpu.VMEM((2, 4, NCH, *CUBE), BF), pltpu.VMEM((2, 256, 512), BF),
        pltpu.VMEM((NCH, 128, WIDE), F32), pltpu.VMEM((NCH, 128, WIDE), F32),
        dma((13,)), dma, dma((4,)), dma, dma((4,)), dma, dma, dma((4,)), dma((4,)), dma((NCH,)), dma((NCH,)),
        dma((2, 3, NCH, 3)), dma((2, 3, NCH, 3)), dma((2, 3, NCH, 3)), dma((2, 3, NCH, 3)), dma((NCH,)), dma((NCH,)),
    ]
    arrays = (ci, gi, go, taps, docs.reshape(4, 128), res, op, gain.reshape(1, 2048), ids.T, wts.T, wg, wu, wd)
    arrays = [pltpu.with_memory_space_constraint(v, pltpu.HBM) for v in arrays]
    return pl.pallas_call(
        layer_kernel,
        out_shape=jax.ShapeDtypeStruct((128, 2048), BF),
        in_specs=[hbm] * 13,
        out_specs=vmem,
        scratch_shapes=scratch,
        compiler_params=pltpu.CompilerParams(
            collective_id=0, has_side_effects=True, vmem_limit_bytes=54000000
        ),
    )(*arrays)


def solution(mesh):
    in_specs = (
        P("sp", "tp"),
        P("sp", "tp"),
        P("sp", "tp"),
        P(None, "tp"),
        P("sp"),
        P(("sp", "tp"), None),
        P(),
        P(),
        P(("sp", "tp"), None),
        P(("sp", "tp"), None),
        P(("sp", "tp"), None, None),
        P(("sp", "tp"), None, None),
        P(("sp", "tp"), None, None),
    )
    out_specs = P(("sp", "tp"), None)
    return jax.shard_map(
        on_device, mesh=mesh, in_specs=in_specs, out_specs=out_specs, check_vma=False
    )
```

```python
import jax
import jax.numpy as jnp
from jax import lax
from jax.experimental import pallas as pl
from jax.experimental.pallas import tpu as pltpu
from jax.sharding import PartitionSpec as P

MESH = pl.DeviceIdType.MESH
BF = jnp.bfloat16
F32 = jnp.float32
WIDTHS = (512, 512, 512, 512)
STARTS = (0, 512, 1024, 1536)
NCH = len(WIDTHS)
WIDE = max(WIDTHS)
CUBE = (2, 4, 4, 8, WIDE)
HALF = 256
STEPS = (1, 3, 2)


def schedule():
    ks = range(NCH)
    order = []
    for p in range(3):
        for w in range(2):
            order += [("D", w, k, p) for k in ks]
    order += [("F", 0, k) for k in ks] + [("C", 0, k, 0) for k in ks]
    order += [("F", 1, k) for k in ks] + [("C", 1, k, 0) for k in ks]
    for p in range(1, 3):
        for w in range(2):
            order += [("C", w, k, p) for k in ks]
    return order + [("E", w, k) for w in range(2) for k in ks]


def layer_kernel(
    ci_h, gi_h, go_h, taps_h, docs_h, res_h, op_h, gain_h, ids_h, wts_h, wg_h, wu_h, wd_h,
    out,
    ci, gi, go, taps, docs, ids, wts, gain, res, opv, wg, wu, wd,
    inner, halo_send, halo_all, fix_send, fix_all, docs8, conv_send, conv_all,
    carried, meta_send, meta, tok, pack, there, gsum, usum, hid, back, comb,
    part_send, part_recv,
    load_sem, halo_s, halo_r, fix_s, fix_r, meta_s, meta_r, tp_send, tp_recv, tok_send, tok_recv,
    d_send, d_recv, c_send, c_recv, p_send, p_recv,
):
    sp = lax.axis_index("sp")
    x = lax.axis_index("tp")
    c = sp % 2
    y = (sp // 2) % 4
    z = sp // 8
    here = [z, y + c * (x - y), x + c * (y - x)]

    def along(axis, step):
        at = list(here)
        at[axis] = (at[axis] + step) % 4
        row, col = at[1] + c * (at[2] - at[1]), at[2] + c * (at[1] - at[2])
        return ((at[0] * 4 + row) * 2 + c, col)

    twin = (sp + 1 - 2 * c, x)
    after = ((sp + 1) % 32, 0)
    tp_far = [(sp, (x + j) % 4) for j in range(4)]

    def load(src, dst, i):
        return pltpu.make_async_copy(src, dst, load_sem.at[i])

    pairs = [(ci_h, ci), (gi_h, gi), (taps_h, taps), (docs_h, docs), (ids_h, ids), (wts_h, wts), (go_h, go),
             (gain_h, gain), (res_h, res), (op_h, opv), (wg_h.at[0], wg), (wu_h.at[0], wu), (wd_h.at[0], wd)]
    loads = [load(src, dst, i) for i, (src, dst) in enumerate(pairs)]
    for i in range(7):
        loads[i].start()

    bar = pltpu.get_barrier_semaphore()
    for axis in range(3):
        for step in STEPS:
            pl.semaphore_signal(bar, inc=1, device_id=along(axis, step), device_id_type=MESH)
    pl.semaphore_signal(bar, inc=1, device_id=twin, device_id_type=MESH)

    @pl.when(x == 0)
    def _():
        for t in range(4):
            pl.semaphore_signal(bar, inc=1, device_id=((sp + 31) % 32, t), device_id_type=MESH)

    for i in range(6):
        loads[i].wait()
    for i in range(7, 13):
        loads[i].start()
    meta_send[0:2, :] = ids[...].astype(F32)
    meta_send[2:4, :] = wts[...]
    docs8[0:1, :] = jnp.full((1, 128), -1, jnp.int32)
    docs8[1:5, :] = docs[...]
    inner[0:8, :] = jnp.zeros((8, 256), F32)
    inner[8:520, :] = ci[...].astype(F32) * gi[...].astype(F32)

    def remote(src, dst, ssem, rsem, dev):
        return pltpu.make_async_remote_copy(
            src_ref=src, dst_ref=dst, send_sem=ssem, recv_sem=rsem, device_id=dev, device_id_type=MESH
        )

    t0 = taps[0:1, :].astype(F32)
    t1 = taps[1:2, :].astype(F32)
    t2 = taps[2:3, :].astype(F32)
    last = docs[3:4, :].astype(F32)
    halo_send[0:1, :] = t1 * inner[519:520, :]
    halo_send[1:2, :] = t0 * inner[518:519, :]
    halo_send[2:3, :] = t0 * inner[519:520, :]
    halo_send[3:4, :] = jnp.broadcast_to(last[:, 127:128], (1, 256))
    halo_send[4:5, :] = jnp.broadcast_to(last[:, 126:127], (1, 256))

    pl.semaphore_wait(bar, 11)
    halo_copy = remote(halo_send, halo_all.at[x], halo_s, halo_r.at[x], after)
    meta_copy = remote(meta_send, meta, meta_s, meta_r, twin)
    halo_copy.start()
    meta_copy.start()

    rows = lax.broadcasted_iota(jnp.int32, (128, 128), 0)
    lanes = lax.broadcasted_iota(jnp.int32, (128, 128), 1)
    eye = jnp.where(rows == lanes, 1.0, 0.0).astype(F32)

    def column(row):
        return jnp.sum(eye * row, axis=1, keepdims=True)

    lane8 = lax.broadcasted_iota(jnp.int32, (8, 128), 1)

    def conv_block(b):
        cur = jnp.broadcast_to(docs8[b + 1 : b + 2, :], (8, 128))
        prev = jnp.broadcast_to(docs8[b : b + 1, :], (8, 128))
        one = jnp.where(lane8 < 1, pltpu.roll(prev, 1, 1), pltpu.roll(cur, 1, 1))
        two = jnp.where(lane8 < 2, pltpu.roll(prev, 2, 1), pltpu.roll(cur, 2, 1))
        m1 = column(jnp.where(one == cur, 1.0, 0.0).astype(F32)[0:1, :])
        m2 = column(jnp.where(two == cur, 1.0, 0.0).astype(F32)[0:1, :])
        base = 8 + 128 * b
        i0 = inner[base : base + 128, :]
        i1 = inner[base - 1 : base + 127, :]
        i2 = inner[base - 2 : base + 126, :]
        value = t2 * i0 + t1 * (m1 * i1) + t0 * (m2 * i2)
        gate = go[128 * b : 128 * b + 128, :].astype(F32)
        conv_send[b] = (gate * value).astype(BF)
        if b == 0:
            fix_send[0:8, :] = value[0:8, :]
            fix_send[8:16, :] = gate[0:8, :]

    def tp_copy(j):
        return remote(conv_send.at[(x + j) % 4], conv_all.at[x], tp_send.at[j], tp_recv.at[j], tp_far[j])

    def fix_copy(t):
        return remote(fix_send, fix_all.at[t], fix_s, fix_r.at[t], (sp, 0))

    loads[6].wait()
    for b in range(4):
        conv_block(b)

    @pl.when(x != 0)
    def _():
        fix_copy(x).start()

    for j in STEPS:
        tp_copy(j).start()
    conv_all[x] = conv_send[x]

    @pl.when(x == 0)
    def _():
        fix_all[0] = fix_send[...]

    meta_copy.wait_recv()

    def routing(table):
        e = [table[a : a + 1, :] for a in range(2)]
        ec = [column(v) for v in e]
        out_rows = []
        for a in range(2):
            same = ((ec[0] == e[a]) | (ec[1] == e[a])) & (rows < lanes)
            rank = jnp.sum(jnp.where(same, 1.0, 0.0).astype(F32), axis=0, keepdims=True)
            ei = e[a].astype(jnp.int32)

            ahead = (((ei >> 5) & 3) - z + 4) & 3
            row, col = (ei >> 3) & 3, ei & 3
            unit = col + c * (row - col) + 4 * (row + c * (col - row)) + 16 * (2 * (ahead & 1) + (ahead >> 1))
            out_rows.append((unit * 8 + rank.astype(jnp.int32), (ei >> 2) & 1))
        return out_rows

    slot_rows = lax.broadcasted_iota(jnp.int32, (512, 128), 0)
    slot_lanes = lax.broadcasted_iota(jnp.int32, (128, 512), 1).astype(F32)
    for s, table in ((0, meta_send), (1, meta)):
        source_core = c if s == 0 else 1 - c
        targets = []
        for slot, parity in routing(table):
            targets.append(jnp.where(parity == c, slot + 4 * source_core, -1))
        hit = (slot_rows == targets[0]) | (slot_rows == targets[1])
        pack[:, 128 * s : 128 * s + 128] = jnp.where(hit, 1.0, 0.0).astype(F32).astype(BF)
        weight = jnp.zeros((128, 512), F32)
        for a in range(2):
            tc = column(targets[a].astype(F32))
            wc = column(table[2 + a : 3 + a, :])
            weight = weight + jnp.where(slot_lanes == tc, wc, 0.0)
        high = weight.astype(BF)
        comb[0, 128 * s : 128 * s + 128, :] = high
        comb[1, 128 * s : 128 * s + 128, :] = (weight - high.astype(F32)).astype(BF)

    for i in (7, 8, 9):
        loads[i].wait()
    for j in range(1, 4):
        pltpu.make_async_remote_copy(
            src_ref=conv_send.at[0], dst_ref=conv_all.at[(x + 4 - j) % 4], send_sem=tp_send.at[j],
            recv_sem=tp_recv.at[j], device_id=tp_far[j], device_id_type=MESH,
        ).wait_recv()

    @pl.when(x == 0)
    def _():
        edge = lax.broadcasted_iota(jnp.int32, (8, 256), 0)
        first = docs[0:1, :].astype(F32)
        inside = jnp.where(sp == 0, 0.0, 1.0)
        for t in range(4):
            if t > 0:
                fix_copy(t).wait_recv()
            remote(halo_send, halo_all.at[t], halo_s, halo_r.at[t], after).wait_recv()
            from_behind = halo_all[t]
            m1 = jnp.where(from_behind[3:4] == first[:, 0:1], inside, 0.0)
            m2 = jnp.where(from_behind[4:5] == first[:, 0:1], inside, 0.0)
            m3 = jnp.where(from_behind[3:4] == first[:, 1:2], inside, 0.0)
            add0 = m1 * from_behind[0:1] + m2 * from_behind[1:2]
            add1 = m3 * from_behind[2:3]
            extra = jnp.where(edge == 0, add0, jnp.where(edge == 1, add1, 0.0))
            fixed = fix_all[t, 8:16, :] * (fix_all[t, 0:8, :] + extra)
            conv_all[t, 0:8, :] = fixed.astype(BF)

    total = jnp.zeros((128, 1), F32)
    for k in range(NCH):
        for n in range(0, WIDTHS[k], 256):
            cols = slice(STARTS[k] + n, STARTS[k] + n + 256)
            acc = jnp.zeros((128, 256), F32)
            for i in range(4):
                acc = acc + jnp.dot(conv_all[i], opv[256 * i : 256 * i + 256, cols], preferred_element_type=F32)
            value = res[:, cols].astype(F32) + acc.astype(BF).astype(F32)
            total = total + jnp.sum(value * value, axis=1, keepdims=True)
            carried[k, :, n : n + 256] = value
    scale = lax.rsqrt(total / 2048.0 + 1e-6)

    def tok_copy(k):
        lanes_k = pl.ds(0, WIDTHS[k])
        return remote(
            tok.at[k, pl.ds(0, 128), lanes_k], tok.at[k, pl.ds(128, 128), lanes_k],
            tok_send.at[k], tok_recv.at[k], twin,
        )

    for k in range(NCH):
        width, start = WIDTHS[k], STARTS[k]
        normed = carried[k, :, :width] * scale * gain[:, start : start + width]
        tok[k, 0:128, :width] = normed.astype(BF)
        tok_copy(k).start()

    def plane(buf, w, p, k, axis, v):
        index = [slice(None)] * 3
        index[axis] = v
        return buf.at[(w, p, k, *index, slice(None), pl.ds(0, WIDTHS[k]))]

    def axis_of(w, p, k):
        return (k + 2 * p + 2 * w) % 3

    def moves(buf, ss, rs, w, p, k, sign):
        axis = axis_of(w, p, k)
        found = []
        if axis == 0:
            for j in range(2):
                step = (w + 2 * j) * sign % 4
                if step != 0:
                    found.append((plane(buf, w, p, k, 0, j), plane(buf, w, p + 1, k, 0, j), step))
        else:
            for step in STEPS:
                source = plane(buf, w, p, k, axis, (here[axis] + step) % 4)
                found.append((source, plane(buf, w, p + 1, k, axis, here[axis]), step))
        return [
            remote(src, dst, ss.at[w, p, k, n], rs.at[w, p, k, n], along(axis, step))
            for n, (src, dst, step) in enumerate(found)
        ]

    def begin(buf, ss, rs, w, p, k, sign):
        for copy in moves(buf, ss, rs, w, p, k, sign):
            copy.start()
        axis = axis_of(w, p, k)
        if axis != 0:
            stay = plane(buf, w, p + 1, k, axis, here[axis])
            stay[...] = plane(buf, w, p, k, axis, here[axis])[...]
        elif w == 0:
            stay = plane(buf, w, p + 1, k, 0, 0)
            stay[...] = plane(buf, w, p, k, 0, 0)[...]

    def settle(buf, ss, rs, w, p, k, sign):
        for copy in moves(buf, ss, rs, w, p, k, sign):
            copy.wait_recv()

    out_way = (there, d_send, d_recv)
    home_way = (back, c_send, c_recv)

    def columns(k):
        return slice(STARTS[k], STARTS[k] + WIDTHS[k])

    def put(buf, w, k, value):
        buf[w, 0, k, :, :, :, :, : WIDTHS[k]] = value.reshape(*CUBE[:4], WIDTHS[k]).astype(BF)

    def rows_of(buf, w, k):
        return buf[w, 3, k, :, :, :, :, : WIDTHS[k]].astype(F32).reshape(HALF, WIDTHS[k]).astype(BF)

    def step_out(w, k, p):
        if p == 0:
            if w == 0:
                tok_copy(k).wait_recv()
            source = tok[k, :, : WIDTHS[k]]
            put(there, w, k, jnp.dot(pack[HALF * w : HALF * w + HALF, :], source, preferred_element_type=F32))
        else:
            settle(*out_way, w, p - 1, k, 1)
        begin(*out_way, w, p, k, 1)

    def gate_up(w, k):
        if w == 0 and k == 0:
            loads[10].wait()
            loads[11].wait()
        settle(*out_way, w, 2, k, 1)
        source = rows_of(there, w, k)
        rows_k = columns(k)
        if k == NCH - 1:
            for n in range(0, 1024, 256):
                block = slice(n, n + 256)
                g = gsum[w, :, block] + jnp.dot(source, wg[rows_k, block], preferred_element_type=F32)
                u = usum[w, :, block] + jnp.dot(source, wu[rows_k, block], preferred_element_type=F32)
                half = 0.5 * g
                hid[w, :, block] = ((half + half * jnp.tanh(half)) * u).astype(BF)
            return
        g = jnp.dot(source, wg[rows_k, :], preferred_element_type=F32)
        u = jnp.dot(source, wu[rows_k, :], preferred_element_type=F32)
        if k == 0:
            gsum[w] = g
            usum[w] = u
        else:
            gsum[w] += g
            usum[w] += u

    def step_home(w, k, p):
        if w == 0 and k == 0 and p == 0:
            loads[12].wait()
        if p == 0:
            put(back, w, k, jnp.dot(hid[w], wd[:, columns(k)], preferred_element_type=F32))
        else:
            settle(*home_way, w, p - 1, k, -1)
        begin(*home_way, w, p, k, -1)

    def part_copy(k):
        part = (k, slice(None), pl.ds(0, WIDTHS[k]))
        return remote(part_send.at[part], part_recv.at[part], p_send.at[k], p_recv.at[k], twin)

    def collect(w, k):
        settle(*home_way, w, 2, k, -1)
        source = rows_of(back, w, k)
        slots = slice(HALF * w, HALF * w + HALF)
        both = jnp.dot(comb[0, :, slots], source, preferred_element_type=F32) + jnp.dot(
            comb[1, :, slots], source, preferred_element_type=F32
        )
        carried[k, :, : WIDTHS[k]] += both[:128]
        if w == 0:
            part_send[k, :, : WIDTHS[k]] = both[128:]
        else:
            part_send[k, :, : WIDTHS[k]] += both[128:]
            part_copy(k).start()

    actions = {"D": step_out, "F": gate_up, "C": step_home, "E": collect}
    for name, *where in schedule():
        actions[name](*where)

    for k in range(NCH):
        part_copy(k).wait_recv()
        width = WIDTHS[k]
        out[:, columns(k)] = (carried[k, :, :width] + part_recv[k, :, :width]).astype(BF)

    halo_copy.wait_send()
    meta_copy.wait_send()

    @pl.when(x != 0)
    def _():
        fix_copy(x).wait_send()

    for w in range(2):
        for p in range(3):
            for k in range(NCH):
                for copy in moves(*out_way, w, p, k, 1) + moves(*home_way, w, p, k, -1):
                    copy.wait_send()
    for j in range(1, 4):
        pltpu.make_async_remote_copy(
            src_ref=conv_send.at[0], dst_ref=conv_all.at[0], send_sem=tp_send.at[j],
            recv_sem=tp_recv.at[j], device_id=tp_far[j], device_id_type=MESH,
        ).wait_send()
    for j in range(NCH):
        tok_copy(j).wait_send()
    for k in range(NCH):
        part_copy(k).wait_send()


def on_device(ci, gi, go, taps, docs, res, op, gain, ids, wts, wg, wu, wd):
    vmem = pl.BlockSpec(memory_space=pltpu.VMEM)
    hbm = pl.BlockSpec(memory_space=pltpu.HBM)
    dma = pltpu.SemaphoreType.DMA
    scratch = [
        pltpu.VMEM((512, 256), BF), pltpu.VMEM((512, 256), BF), pltpu.VMEM((512, 256), BF),
        pltpu.VMEM((3, 256), BF), pltpu.VMEM((4, 128), jnp.int32), pltpu.VMEM((2, 128), jnp.int32),
        pltpu.VMEM((2, 128), F32), pltpu.VMEM((1, 2048), F32),
        pltpu.VMEM((128, 2048), BF), pltpu.VMEM((1024, 2048), BF),
        pltpu.VMEM((2048, 1024), BF), pltpu.VMEM((2048, 1024), BF), pltpu.VMEM((1024, 2048), BF),
        pltpu.VMEM((520, 256), F32), pltpu.VMEM((8, 256), F32), pltpu.VMEM((4, 8, 256), F32),
        pltpu.VMEM((16, 256), F32), pltpu.VMEM((4, 16, 256), F32),
        pltpu.VMEM((8, 128), jnp.int32), pltpu.VMEM((4, 128, 256), BF), pltpu.VMEM((4, 128, 256), BF),
        pltpu.VMEM((NCH, 128, WIDE), F32), pltpu.VMEM((4, 128), F32), pltpu.VMEM((4, 128), F32),
        pltpu.VMEM((NCH, 256, WIDE), BF), pltpu.VMEM((512, 256), BF), pltpu.VMEM((2, 4, NCH, *CUBE), BF),
        pltpu.VMEM((2, HALF, 1024), F32), pltpu.VMEM((2, HALF, 1024), F32), pltpu.VMEM((2, HALF, 1024), BF),
        pltpu.VMEM((2, 4, NCH, *CUBE), BF), pltpu.VMEM((2, 256, 512), BF),
        pltpu.VMEM((NCH, 128, WIDE), F32), pltpu.VMEM((NCH, 128, WIDE), F32),
        dma((13,)), dma, dma((4,)), dma, dma((4,)), dma, dma, dma((4,)), dma((4,)), dma((NCH,)), dma((NCH,)),
        dma((2, 3, NCH, 3)), dma((2, 3, NCH, 3)), dma((2, 3, NCH, 3)), dma((2, 3, NCH, 3)), dma((NCH,)), dma((NCH,)),
    ]
    arrays = (ci, gi, go, taps, docs.reshape(4, 128), res, op, gain.reshape(1, 2048), ids.T, wts.T, wg, wu, wd)
    arrays = [pltpu.with_memory_space_constraint(v, pltpu.HBM) for v in arrays]
    return pl.pallas_call(
        layer_kernel,
        out_shape=jax.ShapeDtypeStruct((128, 2048), BF),
        in_specs=[hbm] * 13,
        out_specs=vmem,
        scratch_shapes=scratch,
        compiler_params=pltpu.CompilerParams(
            collective_id=0, has_side_effects=True, vmem_limit_bytes=54000000
        ),
    )(*arrays)


def solution(mesh):
    in_specs = (
        P("sp", "tp"),
        P("sp", "tp"),
        P("sp", "tp"),
        P(None, "tp"),
        P("sp"),
        P(("sp", "tp"), None),
        P(),
        P(),
        P(("sp", "tp"), None),
        P(("sp", "tp"), None),
        P(("sp", "tp"), None, None),
        P(("sp", "tp"), None, None),
        P(("sp", "tp"), None, None),
    )
    out_specs = P(("sp", "tp"), None)
    return jax.shard_map(
        on_device, mesh=mesh, in_specs=in_specs, out_specs=out_specs, check_vma=False
    )
```
